32 devices in a mesh: sp: 4 (over y, x), tp: 8 (over z, core).
Axes of the slice: x: 2, y: 2, z: 4, core: 2. Of those that a mesh axis runs over, the one named last changes fastest.
Arguments:
- layer_in: bfloat16 [1280, 2048], P('sp', 'tp'), may hold values from -6 to 6
- out_cot: bfloat16 [1280, 2048], P('sp', 'tp'), may hold values from -6 to 6
- route_ids: int32 [1280, 2], P('sp'), may hold values from 0 to 3, all different within a row; in each aligned block of 320 rows (0 to 319, 320 to 639, ...) at most 320 rows name the same one
- route_probs: float32 [1280, 2], P('sp'), may hold values from 0.2 to 1
- group_prob: float32 [1280], P('sp'), may hold values from 0.3 to 1
- gate_weight: bfloat16 [4, 2048, 2048], P('sp', 'tp'), may hold values from -0.125 to 0.125
- up_weight: bfloat16 [4, 2048, 2048], P('sp', 'tp'), may hold values from -0.125 to 0.125
- down_weight: bfloat16 [4, 2048, 2048], P('sp', 'tp'), may hold values from -0.125 to 0.125
- out_weight: bfloat16 [2048, 2048], P(None, 'tp'), may hold values from -0.125 to 0.125
- query: bfloat16 [1280, 1024], P('sp', 'tp'), may hold values from -6 to 6
- key_in: bfloat16 [1280, 1024], P('sp', 'tp'), may hold values from -0.75 to 0.75
- value: bfloat16 [1280, 2048], P('sp', 'tp'), may hold values from -6 to 6
- decay_logit: bfloat16 [1280, 1024], P('sp', 'tp'), may hold values from -2.5 to 8.5, as said below
Outputs:
- gate_grad: float32 [4, 2048, 2048], P('sp', 'tp')
- up_grad: float32 [4, 2048, 2048], P('sp', 'tp')
- down_grad: float32 [4, 2048, 2048], P('sp', 'tp')
- proj_grad: float32 [2048, 2048], P('sp', 'tp')
- query_grad: float32 [1280, 1024], P('sp', 'tp')
- key_grad: float32 [1280, 1024], P('sp', 'tp')
- value_grad: float32 [1280, 2048], P('sp', 'tp')
- logit_grad: float32 [1280, 1024], P('sp', 'tp')
The draws below stay inside these ranges and needn't reach their ends.
Inputs may be any that keep to these rules, and one draw needn't show every extreme that they name: `route_ids`: each row names two different experts of 0 to 3; every expert is named by some row; within each aligned block of 320 rows (the rows of one device) no expert is named more than 320 times, and in some block one expert is named exactly 320 times. `decay_logit`: values lie between -2.5 and 8.5; even heads have pre-activations near 5, odd heads near 1.
All inputs are finite; a program needn't handle non-finite values.
Results may differ from the reference program's by a relative error of at most 0.019.
Values may be sent and summed in bfloat16 or wider, within the bound.
A program may use at most 128 MiB of HBM per device.

```python
import math
import jax
import jax.numpy as jnp
import numpy as np
from jax import lax

D = 2048
FFE = 2048
HEADS = 16
DK = 64
DV = 128
BLOCK = 64
TOK_DEV = 320
TOKENS = 1280
EXPERTS = 4
CAP = 320
N_SP = 4
N_TP = 8


def draw_decay_logit(key, part):
    shift_key, noise_key = jax.random.split(key, 2)
    channel_head = jnp.arange(HEADS * DK) // DK
    base_level = jnp.where(channel_head % 2 == 0, 5.0, 1.0)
    span_shift = jax.random.uniform(shift_key, (TOKENS // TOK_DEV, HEADS), minval=-0.8, maxval=0.8)
    row_span = jnp.arange(TOKENS) // TOK_DEV
    slow_part = span_shift[row_span][:, channel_head]
    noise_part = jnp.clip(0.6 * jax.random.normal(noise_key, (TOKENS, HEADS * DK)), -2.4, 2.4)
    return (base_level[None, :] + slow_part + noise_part).astype(jnp.float32).astype(jnp.bfloat16)


def raised(entries, rng, source, target, blocks, factor):
    owner, partner = [(jnp.arange(entries.shape[axis_at]) // (entries.shape[axis_at] // blocks)).reshape([-1 if axis == axis_at else 1 for axis in range(entries.ndim)]) for axis_at in (source, target)]
    chosen = jax.random.permutation(rng, blocks)[partner]
    strong = (owner == chosen) | (owner == (partner + blocks // 2) % blocks)
    return jnp.where(strong, factor * entries, entries)


def block_scale(rng, shape, cuts, least, largest):
    gain = 1.0
    for position, blocks in cuts:
        draws = jax.random.uniform(jax.random.fold_in(jax.random.fold_in(rng, 6), position), (blocks,), jnp.float32, least / len(cuts), largest / len(cuts))
        gain = gain * jnp.repeat(jnp.exp(draws), shape[position] // blocks).reshape((-1,) + (1,) * (len(shape) - 1 - position))
    return gain


def shared_out(stream_key, own, number, rows, count, top, most, slope):
    sequence = jax.random.permutation(stream_key, count)
    crowded, ordinary = load_shares(count, rows * top, most, slope, True), load_shares(count, rows * top, most, slope, False)
    places = jnp.arange(count)

    def named(sizes, turn):
        used = int((sizes > 0).sum())
        fixed = max(1, used // 4)
        passed = fixed + (places - fixed + turn * (used - fixed)) % max(1, count - fixed)
        return jnp.zeros((count,), jnp.int32).at[sequence[jnp.where(places < fixed, places, passed)]].set(jnp.asarray(sizes, jnp.int32))

    sizes = jnp.where(number % 4 == 0, named(crowded, number // 4), named(ordinary, number - number // 4 - 1))
    mixed = jax.random.permutation(jax.random.fold_in(own, 3), count)
    giver, receiver = mixed[0:count // 2 * 2:2], mixed[1:count // 2 * 2:2]
    room = jnp.minimum(sizes[giver] - 1, most - sizes[receiver]) // 2
    room = jnp.where((giver == sequence[0]) | (receiver == sequence[0]) | (sizes[receiver] == 0), 0, jnp.maximum(room, 0))
    passed = jax.random.randint(jax.random.fold_in(own, 4), (count // 2,), 0, 1 << 20) % (room + 1)
    sizes = sizes.at[giver].add(-passed).at[receiver].add(passed)
    items = jnp.searchsorted(jnp.cumsum(sizes), jnp.arange(rows * top), side="right").astype(jnp.int32)
    grid = items.reshape(top, rows).T
    grid = grid[jax.random.permutation(jax.random.fold_in(own, 1), rows)]
    turn = jax.random.randint(jax.random.fold_in(own, 2), (rows, 1), 0, top)
    return jnp.take_along_axis(grid, (jnp.arange(top)[None, :] + turn) % top, axis=1)


def load_shares(amount, total, reach, skew, full):
    weights = [(1 << 20) // math.isqrt(rank ** skew) + 1 for rank in range(1, amount + 1)]
    largest = reach if full else min(reach, max(-(-total // amount), total * weights[0] // sum(weights)))
    least = 1 if total - largest >= amount - 1 else 0
    given, surplus = [largest] + [least] * (amount - 1), total - largest - least * (amount - 1)
    while surplus > 0:
        candidates = [i for i in range(1, amount) if given[i] < largest] or [i for i in range(1, amount) if given[i] < reach]
        whole, budget = sum([weights[i] for i in candidates]), surplus
        for i in candidates:
            addition = min(reach - given[i], max(1, budget * weights[i] // whole), surplus)
            given[i] = given[i] + addition
            surplus = surplus - addition
    return np.array(given)


def normal_values(rng, dims, deviation, limit, cuts=(), held_as=jnp.bfloat16):
    level = block_scale(rng, dims, cuts, -0.22, 0.18) if cuts else 1.0
    entries = jax.random.normal(rng, dims, jnp.float32) * deviation * level
    return jnp.minimum(jnp.maximum(entries, -limit), limit).astype(held_as)


def noise_with(key, shape, scale, most, cuts, heavy, held_as=jnp.bfloat16):
    drawn = scale * jax.random.normal(key, shape, jnp.float32)
    if cuts:
        drawn = drawn * block_scale(key, shape, cuts, -0.22, 0.18)
    return jnp.clip(raised(drawn, jax.random.fold_in(key, 3), *heavy), -most, most).astype(held_as)


def setup_inputs(seed: int = 0) -> dict:
    streams_of = jax.random.split(jax.random.key(seed), 14)
    layer_in = normal_values(streams_of[0], (TOKENS, D), 1.0, 6.0, ((0, 4), (1, 8)))
    out_cot = noise_with(streams_of[1], (TOKENS, D), 1.0, 6.0, ((0, 4), (1, 8)), (0, 1, 8, 2.0))
    route_ids_keys = jax.random.split(jax.random.fold_in(streams_of[2], 1), TOKENS // TOK_DEV)
    route_ids_turns = jax.random.permutation(jax.random.fold_in(streams_of[2], 3), TOKENS // TOK_DEV)
    route_ids = jax.vmap(lambda own, number: shared_out(jax.random.fold_in(streams_of[2], 2), own, number, TOK_DEV, EXPERTS, 2, CAP, 1))(route_ids_keys, route_ids_turns).reshape((TOKENS, 2))
    route_probs = jnp.clip(0.2 + 0.8 * jax.random.uniform(streams_of[3], (TOKENS, 2), jnp.float32) ** block_scale(streams_of[3], (TOKENS, 2), ((0, 4),), -0.2, 0.2), 0.2, 1.0)
    group_prob = jnp.clip(0.3 + 0.7 * jax.random.uniform(streams_of[4], (TOKENS,), jnp.float32) ** block_scale(streams_of[4], (TOKENS,), ((0, 4),), -0.2, 0.2), 0.3, 1.0)
    gate_weight = normal_values(streams_of[5], (EXPERTS, FFE, D), D ** -0.5, 0.125, ((0, 4), (1, 8)))
    up_weight = normal_values(streams_of[6], (EXPERTS, FFE, D), D ** -0.5, 0.125, ((0, 4), (1, 8)))
    down_weight = normal_values(streams_of[7], (EXPERTS, FFE, D), FFE ** -0.5, 0.125, ((0, 4), (1, 8)))
    out_weight = normal_values(streams_of[8], (D, HEADS * DV), (HEADS * DV) ** -0.5, 0.125, ((1, 8),))
    query = normal_values(streams_of[9], (TOKENS, HEADS * DK), 1.0, 6.0, ((0, 4), (1, 8)))
    key_in = normal_values(streams_of[10], (TOKENS, HEADS * DK), 0.125, 0.75, ((0, 4), (1, 8)))
    value = normal_values(streams_of[11], (TOKENS, HEADS * DV), 1.0, 6.0, ((0, 4), (1, 8)))
    decay_logit = draw_decay_logit(jax.random.fold_in(streams_of[13], 71), 0)
    return dict(layer_in=layer_in, out_cot=out_cot, route_ids=route_ids, route_probs=route_probs, group_prob=group_prob, gate_weight=gate_weight, up_weight=up_weight, down_weight=down_weight, out_weight=out_weight, query=query, key_in=key_in, value=value, decay_logit=decay_logit)


decay_temp = 16.0
highest = lax.Precision.HIGHEST

def mixer_forward(scaled_query, keys_all, values_all, log_decay):
    length_all, head_count, key_dim = scaled_query.shape
    val_dim = values_all.shape[-1]
    blocks = length_all // BLOCK

    def split_blocks(tensor):
        return tensor.reshape(blocks, BLOCK, head_count, tensor.shape[-1]).transpose(2, 0, 1, 3)
    query_blk = split_blocks(scaled_query)
    key_blk = split_blocks(keys_all)
    value_blk = split_blocks(values_all)
    cumulative = jnp.cumsum(split_blocks(log_decay), axis=2)
    span_log = cumulative[:, :, -1:, :]
    query_decayed = query_blk * jnp.exp(cumulative)
    key_back = key_blk * jnp.exp(-cumulative)
    key_to_end = key_blk * jnp.exp(span_log - cumulative)
    causal = jnp.tril(jnp.ones((BLOCK, BLOCK), dtype=bool))
    scores = jnp.where(causal, jnp.einsum('hncd,hnsd->hncs', query_decayed, key_back, precision=highest), 0.0)
    within = jnp.einsum('hncs,hnsv->hncv', scores, value_blk, precision=highest)
    update = jnp.einsum('hncd,hncv->hndv', key_to_end, value_blk, precision=highest)
    block_decay = jnp.exp(span_log[:, :, 0, :])

    def advance(carry_state, inputs):
        decay_now, update_now = inputs
        return (carry_state * decay_now[..., None] + update_now, carry_state)
    start_state = jnp.zeros((head_count, key_dim, val_dim), jnp.float32)
    _, entering = lax.scan(advance, start_state, (jnp.moveaxis(block_decay, 1, 0), jnp.moveaxis(update, 1, 0)))
    entering = jnp.moveaxis(entering, 0, 1)
    carried = jnp.einsum('hncd,hndv->hncv', query_decayed, entering, precision=highest)
    return (within + carried).transpose(1, 2, 0, 3).reshape(length_all, head_count * val_dim)

def reference(layer_in, out_cot, route_ids, route_probs, group_prob, gate_weight, up_weight, down_weight, out_weight, query, key_in, value, decay_logit):
    length_all = layer_in.shape[0]
    width = layer_in.shape[1]
    route_weight = group_prob[:, None] * route_probs / lax.optimization_barrier(jnp.sum(route_probs, axis=1, keepdims=True))
    scaled_cot = (route_weight[:, :, None] * out_cot.astype(jnp.float32)[:, None, :]).astype(jnp.bfloat16)
    flat_ids = route_ids.reshape(-1)
    flat_cot = scaled_cot.reshape(-1, width)
    rows_max = N_SP * CAP
    hidden_dev = FFE // N_TP

    def one_expert(expert):
        order_rows = jnp.argsort((flat_ids != expert).astype(jnp.int32), stable=True)[:rows_max]
        valid_rows = flat_ids[order_rows] == expert
        token_rows = (order_rows // 2).astype(jnp.int32)
        inputs_x = layer_in[token_rows]
        cot_rows = jnp.where(valid_rows[:, None], flat_cot[order_rows], jnp.zeros((), jnp.bfloat16))
        gate_mat = gate_weight[expert]
        up_mat = up_weight[expert]
        down_mat = down_weight[expert]
        gate_pre = jnp.dot(inputs_x, gate_mat.T, preferred_element_type=jnp.float32)
        up_pre = jnp.dot(inputs_x, up_mat.T, preferred_element_type=jnp.float32)
        sigmoid_gate = jax.nn.sigmoid(gate_pre)
        active = gate_pre * sigmoid_gate
        hidden = (active * up_pre).astype(jnp.bfloat16)
        hidden_cot = jnp.dot(cot_rows, down_mat.T, preferred_element_type=jnp.float32)
        up_cot = (hidden_cot * active).astype(jnp.bfloat16)
        gate_cot = (hidden_cot * up_pre * sigmoid_gate * (1.0 + gate_pre * (1.0 - sigmoid_gate))).astype(jnp.bfloat16)
        down_g = jnp.dot(hidden.T, cot_rows, preferred_element_type=jnp.float32)
        gate_g = jnp.dot(gate_cot.T, inputs_x, preferred_element_type=jnp.float32)
        up_g = jnp.dot(up_cot.T, inputs_x, preferred_element_type=jnp.float32)
        gate_groups = gate_cot.astype(jnp.float32).reshape(rows_max, N_TP, hidden_dev)
        up_groups = up_cot.astype(jnp.float32).reshape(rows_max, N_TP, hidden_dev)
        gate_split = gate_mat.astype(jnp.float32).reshape(N_TP, hidden_dev, width)
        up_split = up_mat.astype(jnp.float32).reshape(N_TP, hidden_dev, width)
        partial_sum = jnp.einsum('rjf,jfd->rjd', gate_groups, gate_split, precision=highest)
        partial_sum = partial_sum + jnp.einsum('rjf,jfd->rjd', up_groups, up_split, precision=highest)
        rounded = lax.optimization_barrier(partial_sum.astype(jnp.bfloat16)).astype(jnp.float32)
        input_grad = lax.optimization_barrier(jnp.sum(rounded, axis=1))
        return (gate_g, up_g, down_g, input_grad, token_rows)
    gate_grad, up_grad, down_grad, input_grads, token_index = lax.map(one_expert, jnp.arange(EXPERTS, dtype=jnp.int32))
    routed_sum = jax.ops.segment_sum(input_grads.reshape(-1, width), token_index.reshape(-1), num_segments=length_all)
    mixed_cot = (out_cot.astype(jnp.float32) + routed_sum).astype(jnp.bfloat16)
    mixer_cot = jnp.dot(mixed_cot, out_weight, preferred_element_type=jnp.float32)

    def forward(query_f, key_f, value_f, logit_f):
        scaled = query_f.reshape(length_all, HEADS, DK) * DK ** (-0.5)
        log_decay = (jax.nn.log_sigmoid(logit_f) / decay_temp).reshape(length_all, HEADS, DK)
        return mixer_forward(scaled, key_f.reshape(length_all, HEADS, DK), value_f.reshape(length_all, HEADS, DV), log_decay)
    mixer_f32, pullback = jax.vjp(forward, query.astype(jnp.float32), key_in.astype(jnp.float32), value.astype(jnp.float32), decay_logit.astype(jnp.float32))
    query_grad, key_grad, value_grad, logit_grad = pullback(mixer_cot)
    mixer_out = mixer_f32.astype(jnp.bfloat16)
    proj_grad = jnp.dot(mixed_cot.T, mixer_out, preferred_element_type=jnp.float32)
    return (gate_grad, up_grad, down_grad, proj_grad, query_grad, key_grad, value_grad, logit_grad)
```

```python
import functools
import jax
import jax.numpy as jnp
from jax import lax
from jax.experimental import pallas as pl
from jax.experimental.pallas import tpu as pltpu
from jax.sharding import PartitionSpec as P

DK = 64
DV = 128
BLOCK = 64


decay_temp = 16.0
highest = lax.Precision.HIGH


def prefix(x, axis, join, neutral, backward):
    count = lax.axis_size(axis)
    place = lax.axis_index(axis)
    ahead = count - 1 - place if backward else place
    gathered = jax.tree.map(
        lambda a, kind: lax.all_gather(a.astype(kind), axis),
        x,
        jax.tree.map(lambda a: jnp.bfloat16 if a.dtype == jnp.float32 else a.dtype, x),
    )
    state = jax.tree.map(lambda a, e: jnp.zeros_like(a) + jnp.asarray(e, a.dtype), x, neutral)

    def one(step, state):
        source = count - 1 - step if backward else step
        return join(
            state,
            jax.tree.map(
                lambda a, own: lax.dynamic_index_in_dim(a, source, 0, False).astype(own.dtype),
                gathered,
                x,
            ),
        )

    return lax.fori_loop(0, ahead, one, state)


def combine_spans(earlier, later):
    return (earlier[0] * later[0], later[1] + later[0][..., None] * earlier[1])


def contract_rows(left_mat, right_mat):
    return lax.dot_general(
        left_mat, right_mat, (((0,), (0,)), ((), ())), preferred_element_type=jnp.float32
    )


def contract_cols(left_mat, right_mat):
    return lax.dot_general(
        left_mat, right_mat, (((1,), (1,)), ((), ())), preferred_element_type=jnp.float32
    )


def to_blocks(tensor, head_count):
    rows_here = tensor.shape[0]
    return (
        tensor.astype(jnp.float32)
        .reshape(rows_here // BLOCK, BLOCK, head_count, -1)
        .transpose(2, 0, 1, 3)
    )


def from_blocks(tensor):
    head_count, blocks, _, channels = tensor.shape
    return tensor.transpose(1, 2, 0, 3).reshape(blocks * BLOCK, head_count * channels)


def expert_pass(rows_x, rows_cot, gate_mat, up_mat, down_mat):
    full_x, full_cot = (
        lax.all_gather(rows_x, "tp", axis=1, tiled=True),
        lax.all_gather(rows_cot, "tp", axis=1, tiled=True),
    )
    gate_pre = contract_cols(full_x, gate_mat)
    up_pre = contract_cols(full_x, up_mat)
    sigmoid_gate = jax.nn.sigmoid(gate_pre)
    active = gate_pre * sigmoid_gate
    hidden = (active * up_pre).astype(jnp.bfloat16)
    hidden_cot = contract_cols(full_cot, down_mat)
    up_cot = (hidden_cot * active).astype(jnp.bfloat16)
    gate_cot = (
        hidden_cot * up_pre * sigmoid_gate * (1.0 + gate_pre * (1.0 - sigmoid_gate))
    ).astype(jnp.bfloat16)
    down_g = contract_rows(hidden, full_cot)
    gate_g = contract_rows(gate_cot, full_x)
    up_g = contract_rows(up_cot, full_x)
    dims = (((0,), (1,)), ((), ()))
    first_part = lax.dot_general(gate_mat, gate_cot, dims, preferred_element_type=jnp.float32)
    back_terms = lax.psum_scatter(
        (
            first_part + lax.dot_general(up_mat, up_cot, dims, preferred_element_type=jnp.float32)
        ).astype(jnp.bfloat16),
        "tp",
        scatter_dimension=0,
        tiled=True,
    ).astype(jnp.float32)
    return (gate_g, up_g, down_g, back_terms)


def local(
    layer_in,
    out_cot,
    route_ids,
    route_probs,
    group_prob,
    gate_weight,
    up_weight,
    down_weight,
    out_weight,
    query,
    key_in,
    value,
    decay_logit,
):
    tok_rows = layer_in.shape[0]
    local_cols = layer_in.shape[1]
    experts_all = lax.axis_size("sp")
    capacity = 4 * tok_rows // experts_all
    route_weight = group_prob[:, None] * route_probs / jnp.sum(route_probs, axis=1, keepdims=True)
    chosen = (route_ids[:, :, None] == jnp.arange(experts_all, dtype=jnp.int32)).astype(jnp.int32)
    running = jnp.cumsum(chosen.reshape(2 * tok_rows, experts_all), axis=0).reshape(
        tok_rows, 2, experts_all
    )
    position = jnp.sum((running - 1) * chosen, axis=2)
    slot_ids = route_ids * capacity + position
    matches = (
        slot_ids[None, :, :] == jnp.arange(experts_all * capacity, dtype=jnp.int32)[:, None, None]
    )
    select_x = jnp.any(matches, axis=2).astype(jnp.float32)
    select_cot = jnp.sum(jnp.where(matches, route_weight[None], 0.0), axis=2)
    send_x = jnp.dot(
        select_x.astype(jnp.bfloat16), layer_in, preferred_element_type=jnp.float32
    ).astype(jnp.bfloat16)
    send_cot = jnp.dot(select_cot, out_cot.astype(jnp.float32), precision=highest).astype(
        jnp.bfloat16
    )
    send_x = send_x.reshape(experts_all, capacity, local_cols)
    send_cot = send_cot.reshape(experts_all, capacity, local_cols)
    recv_x, recv_cot = (
        lax.all_to_all(send_x, "sp", split_axis=0, concat_axis=0, tiled=True),
        lax.all_to_all(send_cot, "sp", split_axis=0, concat_axis=0, tiled=True),
    )
    head_dev = query.shape[1] // DK
    scaled_query = to_blocks(query, head_dev) * DK ** (-0.5)
    key_blk = to_blocks(key_in, head_dev)
    value_blk = to_blocks(value, head_dev)
    logit_blk = to_blocks(decay_logit, head_dev)
    cumulative = jnp.cumsum(jax.nn.log_sigmoid(logit_blk) / decay_temp, axis=2)
    span_log = cumulative[:, :, -1:, :]
    growth = jnp.exp(cumulative)
    shrink = jnp.exp(-cumulative)
    to_end = jnp.exp(span_log - cumulative)
    query_decayed = scaled_query * growth
    key_back = key_blk * shrink
    key_to_end = key_blk * to_end
    causal = jnp.tril(jnp.ones((BLOCK, BLOCK), dtype=bool))
    scores = jnp.where(
        causal, jnp.einsum("hncd,hnsd->hncs", query_decayed, key_back, precision=highest), 0.0
    )
    within = jnp.einsum("hncs,hnsv->hncv", scores, value_blk, precision=highest)
    block_decay = jnp.moveaxis(jnp.exp(span_log[:, :, 0, :]), 1, 0)
    block_update = jnp.moveaxis(
        jnp.einsum("hncd,hncv->hndv", key_to_end, value_blk, precision=highest), 1, 0
    )
    identity_pair = (
        jnp.ones((head_dev, DK), jnp.float32),
        jnp.zeros((head_dev, DK, DV), jnp.float32),
    )

    def advance(carry_pair, inputs):
        return (combine_spans(carry_pair, inputs), carry_pair)

    span_total, before_pairs = lax.scan(advance, identity_pair, (block_decay, block_update))
    entry_pair = prefix(span_total, "sp", combine_spans, identity_pair, False)
    entry_state = entry_pair[1]
    decay_before = jnp.moveaxis(before_pairs[0], 0, 1)
    block_state = decay_before[..., None] * entry_state[:, None] + jnp.moveaxis(
        before_pairs[1], 0, 1
    )
    span_end = span_total[0][..., None] * entry_state + span_total[1]
    outputs = within + jnp.einsum("hncd,hndv->hncv", query_decayed, block_state, precision=highest)
    mixer_out = from_blocks(outputs).astype(jnp.bfloat16)
    gate_mat, up_mat, down_mat = (gate_weight[0], up_weight[0], down_weight[0])
    gate_g, up_g, down_g, back_flat = expert_pass(
        recv_x.reshape(-1, local_cols), recv_cot.reshape(-1, local_cols), gate_mat, up_mat, down_mat
    )
    back_terms = back_flat.reshape(local_cols, experts_all, capacity)
    returned = lax.all_to_all(
        back_terms.astype(jnp.bfloat16), "sp", split_axis=1, concat_axis=1, tiled=True
    ).astype(back_terms.dtype)
    returned = returned.reshape(local_cols, experts_all * capacity)
    routed_sum = lax.dot_general(
        select_x,
        returned,
        (((0,), (1,)), ((), ())),
        precision=highest,
        preferred_element_type=jnp.float32,
    )
    mixed_cot = (out_cot.astype(jnp.float32) + routed_sum).astype(jnp.bfloat16)
    full_cot = lax.all_gather(mixed_cot, "tp", axis=1, tiled=True)
    mixer_cot = jnp.dot(full_cot, out_weight, preferred_element_type=jnp.float32)
    proj_grad = lax.psum_scatter(
        contract_rows(full_cot, mixer_out).astype(jnp.bfloat16),
        "sp",
        scatter_dimension=0,
        tiled=True,
    ).astype(jnp.float32)
    cot_blk = to_blocks(mixer_cot, head_dev)
    block_future = jnp.moveaxis(
        jnp.einsum("hncd,hncv->hndv", query_decayed, cot_blk, precision=highest), 1, 0
    )

    def retreat(carry_pair, inputs):
        return (combine_spans(carry_pair, inputs), carry_pair)

    span_back, after_pairs = lax.scan(
        retreat, identity_pair, (block_decay, block_future), reverse=True
    )
    beyond_pair = prefix(span_back, "sp", combine_spans, identity_pair, True)
    future_state = beyond_pair[1]
    decay_after = jnp.moveaxis(after_pairs[0], 0, 1)
    block_future_state = decay_after[..., None] * future_state[:, None] + jnp.moveaxis(
        after_pairs[1], 0, 1
    )
    cot_values = jnp.where(
        causal, jnp.einsum("hncv,hnsv->hncs", cot_blk, value_blk, precision=highest), 0.0
    )
    query_scaled_grad = growth * (
        jnp.einsum("hncv,hndv->hncd", cot_blk, block_state, precision=highest)
        + jnp.einsum("hncs,hnsd->hncd", cot_values, key_back, precision=highest)
    )
    key_part = shrink * jnp.einsum("hncs,hncd->hnsd", cot_values, query_decayed, precision=highest)
    key_grad = key_part + to_end * jnp.einsum(
        "hnsv,hndv->hnsd", value_blk, block_future_state, precision=highest
    )
    value_grad = jnp.einsum("hncs,hncv->hnsv", scores, cot_blk, precision=highest) + jnp.einsum(
        "hnsd,hndv->hnsv", key_to_end, block_future_state, precision=highest
    )
    decay_terms = (scaled_query * query_scaled_grad - key_blk * key_grad).reshape(
        head_dev, tok_rows, DK
    )
    tail_sum = jnp.flip(jnp.cumsum(jnp.flip(decay_terms, 1), axis=1), 1)
    beyond_term = jnp.sum(future_state * span_end, axis=2)
    log_grad = tail_sum + beyond_term[:, None, :]
    logit_flat = logit_blk.reshape(head_dev, tok_rows, DK)
    logit_grad = (
        (log_grad * jax.nn.sigmoid(-logit_flat) / decay_temp)
        .transpose(1, 0, 2)
        .reshape(tok_rows, head_dev * DK)
    )
    query_grad = from_blocks(query_scaled_grad * DK ** (-0.5))
    return (
        gate_g[None],
        up_g[None],
        down_g[None],
        proj_grad,
        query_grad,
        from_blocks(key_grad),
        from_blocks(value_grad),
        logit_grad,
    )


RING = 4
EXPERT_CUT = 5


def ring_place(index):
    return index + (index // 2) * (1 - 2 * (index % 2))


def remote(source, target, send_sem, recv_sem, device):
    return pltpu.make_async_remote_copy(
        src_ref=source,
        dst_ref=target,
        send_sem=send_sem,
        recv_sem=recv_sem,
        device_id=device,
        device_id_type=pl.DeviceIdType.MESH,
    )


def greet(devices):
    barrier = pltpu.get_barrier_semaphore()
    for device in devices:
        pl.semaphore_signal(
            barrier, inc=1, device_id=device, device_id_type=pl.DeviceIdType.MESH
        )
    pl.semaphore_wait(barrier, len(devices))


def arrived(sem, region):
    pltpu.make_async_copy(region, region, sem).wait()


class Place:
    def __init__(self):
        self.sp, self.tp = lax.axis_index("sp"), lax.axis_index("tp")
        self.z, self.core = self.tp // 2, self.tp % 2
        ring = ring_place(self.sp)
        self.at = [ring_place((ring + step) % RING) for step in range(RING)]
        self.right, self.across, self.left = [(self.at[s], self.tp) for s in (1, 2, 3)]
        self.pair = (self.sp, 2 * self.z + 1 - self.core)
        self.near = (self.sp, 2 * (self.z + 1 - 2 * (self.z % 2)) + self.core)
        self.far = (self.sp, 2 * (RING - 1 - self.z) + self.core)
        upper = self.z // 2
        folded = self.z + upper * (RING - 1 - 2 * self.z)
        self.inner = folded == 1
        self.end = folded == 0
        order = [folded, 1 - folded, 2, 3]
        self.slot = [o + upper * (RING - 1 - 2 * o) for o in order]


def expert_kernel(
    x_ref, cot_ref, small_ref, state_ref, gate_ref, up_ref, down_ref,
    gate_out, up_out, down_out, mixed_out, small_out, state_out,
    x_all, cot_all, gate_pre, up_pre, hidden, gate_cot, up_cot,
    pair_to, pair_from, parts, first_in, second_in, total, half_total, z_in,
    tiny_send, tiny_recv, zs, zr, ps, pr, qs, qr,
    bs, br, r1s, r1r, r2s, r2r, zts, ztr, ms, mr,
):
    here = Place()
    tok_rows, width = x_ref.shape
    lead = tok_rows * 4 // EXPERT_CUT
    tail = tok_rows - lead
    ins, alls = (x_ref, cot_ref), (x_all, cot_all)
    greet([here.right, here.across, here.left, here.near, here.far, here.pair])
    plain, guarded = [], []

    def go(source, target, send_sem, recv_sem, device):
        copy = remote(source, target, send_sem, recv_sem, device)
        copy.start()
        plain.append(copy)

    def go_if(cond, source, target, send_sem, recv_sem, device):
        copy = remote(source, target, send_sem, recv_sem, device)

        @pl.when(cond)
        def _():
            copy.start()

        guarded.append((cond, copy))

    def cols(slot, core):
        return pl.ds(pl.multiple_of((2 * here.slot[slot] + core) * width, width), width)

    def piece(a, part, slot, core=None):
        core = here.core if core is None else core
        if part == 0:
            return alls[a].at[here.sp, pl.ds(0, lead), cols(slot, core)]
        return alls[a].at[:, pl.ds(lead, tail), cols(slot, core)]

    def own_rows(a, start, count):
        return ins[a].at[pl.ds(start, count), :]

    def z_start(a, part):
        source = own_rows(a, 0, lead) if part == 0 else piece(a, 1, 0)
        target = piece(a, part, 0)
        go(source, target, zs.at[a, part, 0], zr.at[a, part, 0], here.near)
        go_if(here.inner, source, target, zs.at[a, part, 1], zr.at[a, part, 1], here.far)

    def z_relay(a, part, slot):
        region = piece(a, part, slot)
        arrived(zr.at[a, part, slot - 1], region)
        if slot == 1:
            go_if(here.inner, region, region, zs.at[a, part, 2], zr.at[a, part, 2], here.far)
        else:
            go_if(
                here.inner, region, region, zs.at[a, part, slot + 1], zr.at[a, part, slot - 1],
                here.near,
            )
        if part == 0:
            pair_send(a, slot, 0)
        else:
            go(region, region, qs.at[a, slot, 4], qr.at[a, slot, 4], here.pair)

    def bounds(part, h):
        start, count = (0, lead) if part == 0 else (lead, tail)
        return start + h * (count // 2), count // 2

    def ring_region(a, unit, step, h):
        slot, part = unit
        start, count = bounds(part, h)
        return alls[a].at[here.at[step], pl.ds(start, count), cols(slot, here.core)]

    def number(unit):
        return unit[0] + 4 * unit[1]

    def ring_send(a, unit):
        slot, part = unit
        n = number(unit)
        for h, right_first in ((0, True), (1, False)):
            pass
        for i, (h, device) in enumerate(
            ((0, here.right), (1, here.right), (0, here.left), (1, here.left))
        ):
            start, count = bounds(part, h)
            source = own_rows(a, start, count) if slot == 0 else ring_region(a, unit, 0, h)
            copy = remote(source, ring_region(a, unit, 0, h), ps.at[a, n, i], pr.at[a, n, i], device)
            plain.append(copy)
        right0, right1, left0, left1 = plain[-4:]
        for copy in (right0, left1, right1, left0):
            copy.start()

    def ring_forward(a, unit):
        n = number(unit)
        region = ring_region(a, unit, 3, 0)
        arrived(pr.at[a, n, 0], region)
        go(region, region, ps.at[a, n, 4], pr.at[a, n, 4], here.right)
        region = ring_region(a, unit, 1, 1)
        arrived(pr.at[a, n, 3], region)
        go(region, region, ps.at[a, n, 5], pr.at[a, n, 5], here.left)

    def ring_finish(a, unit):
        n = number(unit)
        arrived(pr.at[a, n, 1], ring_region(a, unit, 3, 1))
        arrived(pr.at[a, n, 2], ring_region(a, unit, 1, 0))
        arrived(pr.at[a, n, 4], ring_region(a, unit, 2, 0))
        arrived(pr.at[a, n, 5], ring_region(a, unit, 2, 1))
        if unit[1] == 0:
            for step in (1, 3, 2):
                pair_send(a, unit[0], step)
        else:
            z_start(a, 1)
            region = piece(a, 1, 0)
            go(region, region, qs.at[a, 0, 4], qr.at[a, 0, 4], here.pair)

    def pair_region(a, slot, step, core):
        return alls[a].at[here.at[step], pl.ds(0, lead), cols(slot, core)]

    def pair_send(a, slot, step):
        region = pair_region(a, slot, step, here.core)
        source = own_rows(a, 0, lead) if slot == 0 and step == 0 else region
        go(source, region, qs.at[a, slot, step], qr.at[a, slot, step], here.pair)

    def pair_wait(a, part):
        for slot in range(RING):
            if part == 0:
                for step in range(RING):
                    arrived(qr.at[a, slot, step], pair_region(a, slot, step, 1 - here.core))
            else:
                arrived(qr.at[a, slot, 4], piece(a, 1, slot, 1 - here.core))

    for a in range(2):
        z_start(a, 0)
    ring_send(0, (0, 0))
    for ref, out, i in ((small_ref, small_out, 0), (state_ref, state_out, 1)):
        for step, device in ((1, here.right), (3, here.left), (2, here.across)):
            go(
                ref, out.at[here.sp], tiny_send.at[i, step - 1], tiny_recv.at[i, 3 - step], device
            )
    ring_send(0, (0, 1))
    ring_send(1, (0, 1))
    for a in range(2):
        alls[a][here.sp, :, cols(0, here.core)] = ins[a][...]
        pair_send(a, 0, 0)
    small_out[here.sp] = small_ref[...]
    state_out[here.sp] = state_ref[...]
    z_relay(0, 0, 1)
    ring_send(0, (1, 0))
    ring_forward(0, (0, 0))
    ring_forward(0, (0, 1))
    ring_forward(1, (0, 1))
    z_relay(0, 0, 2)
    ring_send(0, (2, 0))
    ring_forward(0, (1, 0))
    ring_finish(0, (0, 0))
    z_relay(0, 0, 3)
    ring_send(0, (3, 0))
    ring_forward(0, (2, 0))
    ring_finish(0, (1, 0))
    z_relay(1, 0, 1)
    ring_send(1, (0, 0))
    ring_send(1, (1, 0))
    ring_forward(0, (3, 0))
    ring_finish(0, (2, 0))
    z_relay(1, 0, 2)
    ring_send(1, (2, 0))
    ring_finish(0, (0, 1))
    z_relay(1, 0, 3)
    ring_send(1, (3, 0))
    ring_finish(1, (0, 1))
    ring_forward(1, (0, 0))
    ring_finish(0, (3, 0))
    pair_wait(0, 0)

    def forward_rows(s, start, count):
        rows = pl.ds(start, count)
        block = x_all[s, rows, :]
        gate_pre[s, rows, :] = contract_cols(block, gate_ref[...])
        up_pre[s, rows, :] = contract_cols(block, up_ref[...])

    half = lead // 2
    steps = [
        lambda: ring_forward(1, (1, 0)),
        lambda: z_relay(0, 1, 1),
        lambda: ring_finish(1, (0, 0)),
        lambda: z_relay(0, 1, 2),
        lambda: ring_forward(1, (2, 0)),
        lambda: ring_finish(1, (1, 0)),
        lambda: z_relay(0, 1, 3),
        lambda: ring_forward(1, (3, 0)),
    ]
    for i in range(8):
        forward_rows(i // 2, (i % 2) * half, half)
        steps[i]()
    for s in range(RING):
        for step in (1, 2, 3):
            pass
    for step in (1, 2, 3):
        arrived(tiny_recv.at[0, step - 1], small_out.at[here.at[step]])
        arrived(tiny_recv.at[1, step - 1], state_out.at[here.at[step]])
    ring_finish(1, (2, 0))
    z_relay(1, 1, 1)
    pair_wait(0, 1)
    for s in range(RING):
        forward_rows(s, lead, tail)
    z_relay(1, 1, 2)
    z_relay(1, 1, 3)
    ring_finish(1, (3, 0))
    pair_wait(1, 0)

    pick = (
        lax.broadcasted_iota(jnp.int32, (small_ref.shape[0], 128), 0) == here.sp
    ).astype(jnp.float32)

    def second_rows(s, start, count):
        rows = pl.ds(start, count)
        weight = lax.dot_general(
            small_out[s, :, pl.ds(0, tok_rows)][:, start : start + count],
            pick,
            (((0,), (0,)), ((), ())),
            precision=lax.Precision.HIGHEST,
            preferred_element_type=jnp.float32,
        )
        weight = jnp.concatenate([weight] * (width // 128), axis=1)
        hidden_cot = contract_cols(cot_all[s, rows, :], down_ref[...]) * weight
        gp, upp = gate_pre[s, rows, :], up_pre[s, rows, :]
        sig = 1.0 / (1.0 + jnp.exp(-gp))
        active = gp * sig
        hidden[s, rows, :] = (active * upp * weight).astype(jnp.bfloat16)
        up_cot[s, rows, :] = (hidden_cot * active).astype(jnp.bfloat16)
        gate_cot[s, rows, :] = (hidden_cot * upp * sig * (1.0 + gp * (1.0 - sig))).astype(
            jnp.bfloat16
        )

    for i in range(8):
        second_rows(i // 2, (i % 2) * half, half)
    pair_wait(1, 1)
    for s in range(RING):
        second_rows(s, lead, tail)

    pieces, wide = parts.shape[0], parts.shape[3]
    split = tok_rows // 2
    per = width // wide

    def back_cols(k, core):
        at = (2 * (k // per) + core) * width + (k % per) * wide
        return pl.ds(pl.multiple_of(at, wide), wide)

    def partial(k, step, core):
        c = back_cols(k, core)
        s = here.at[step]
        return jnp.dot(
            gate_cot[s], gate_ref[:, c], preferred_element_type=jnp.float32
        ) + jnp.dot(up_cot[s], up_ref[:, c], preferred_element_type=jnp.float32)

    ring_order = (2, 1, 3, 0)

    def pair_part(k):
        for step in ring_order:
            pair_to[k, step] = partial(k, step, 1 - here.core).astype(jnp.bfloat16)
            go(
                pair_to.at[k, step], pair_from.at[k, step], bs.at[k, step], br.at[k, step], here.pair
            )

    top, bottom = pl.ds(0, split), pl.ds(split, split)

    def own_part(k):
        for step in ring_order:
            mine = partial(k, step, here.core)
            arrived(br.at[k, step], pair_from.at[k, step])
            parts[k, step] = (mine + pair_from[k, step].astype(jnp.float32)).astype(jnp.bfloat16)
            if step == 2:
                go(parts.at[k, 2, top], first_in.at[k, 0], r1s.at[k, 0], r1r.at[k, 0], here.right)
                go(parts.at[k, 2, bottom], first_in.at[k, 1], r1s.at[k, 1], r1r.at[k, 1], here.left)
            if step == 1:
                go(
                    parts.at[k, 1, bottom], second_in.at[k, 0, bottom],
                    r2s.at[k, 0], r2r.at[k, 0], here.right,
                )
            if step == 3:
                go(
                    parts.at[k, 3, top], second_in.at[k, 1, top],
                    r2s.at[k, 1], r2r.at[k, 1], here.left,
                )

    def add_to(ref, other):
        ref[...] = (ref[...].astype(jnp.float32) + other.astype(jnp.float32)).astype(jnp.bfloat16)

    def ring_relay(k):
        arrived(r1r.at[k, 0], first_in.at[k, 0])
        add_to(parts.at[k, 1, top], first_in[k, 0])
        go(
            parts.at[k, 1, top], second_in.at[k, 0, top], r2s.at[k, 2], r2r.at[k, 2], here.right
        )
        arrived(r1r.at[k, 1], first_in.at[k, 1])
        add_to(parts.at[k, 3, bottom], first_in[k, 1])
        go(
            parts.at[k, 3, bottom], second_in.at[k, 1, bottom],
            r2s.at[k, 3], r2r.at[k, 3], here.left,
        )

    def ring_total(k):
        arrived(r2r.at[k, 0], second_in.at[k, 0, bottom])
        arrived(r2r.at[k, 1], second_in.at[k, 1, top])
        arrived(r2r.at[k, 2], second_in.at[k, 0, top])
        arrived(r2r.at[k, 3], second_in.at[k, 1, bottom])
        total[k] = (
            parts[k, 0].astype(jnp.float32)
            + second_in[k, 0].astype(jnp.float32)
            + second_in[k, 1].astype(jnp.float32)
        ).astype(jnp.bfloat16)
        go_if(here.end, total.at[k], z_in.at[k, 0], zts.at[k, 0], ztr.at[k, 0], here.near)

    def line_middle(k):
        copy = remote(half_total.at[k], z_in.at[k, 1], zts.at[k, 1], ztr.at[k, 1], here.far)

        @pl.when(here.inner)
        def _():
            arrived(ztr.at[k, 0], z_in.at[k, 0])
            half_total[k] = (
                total[k].astype(jnp.float32) + z_in[k, 0].astype(jnp.float32)
            ).astype(jnp.bfloat16)
            copy.start()

        guarded.append((here.inner, copy))

    def line_total(k):
        c = back_cols(k, here.core)
        region = mixed_out.at[:, c]
        copy = remote(region, region, ms.at[k, 0], mr.at[k, 0], here.near)

        @pl.when(here.inner)
        def _():
            arrived(ztr.at[k, 1], z_in.at[k, 1])
            mixed_out[:, c] = (
                cot_all[here.sp, :, c].astype(jnp.float32)
                + (half_total[k].astype(jnp.float32) + z_in[k, 1].astype(jnp.float32))
            ).astype(jnp.bfloat16)
            copy.start()

        guarded.append((here.inner, copy))

        @pl.when(here.end)
        def _():
            arrived(mr.at[k, 0], region)

        go(region, region, ms.at[k, 1], mr.at[k, 1], here.pair)

    features = gate_ref.shape[1]
    blocks = features // width

    def weight_grad(n):
        which, j = n // blocks, n % blocks
        left, right, out = (
            (gate_cot, x_all, gate_out), (up_cot, x_all, up_out), (hidden, cot_all, down_out)
        )[which]
        c = pl.ds(j * width, width)
        rows = RING * tok_rows
        out[:, c] = contract_rows(
            left[...].reshape(rows, width), right[:, :, c].reshape(rows, width)
        )

    grads = list(range(3 * blocks))

    def some_grads(count):
        for _ in range(min(count, len(grads))):
            weight_grad(grads.pop(0))

    lanes = []
    pair_part(0)
    for k in range(pieces + 5):
        if k + 1 < pieces:
            pair_part(k + 1)
        if k < pieces:
            own_part(k)
        some_grads(-(-3 * blocks // (pieces + 4)))
        if 0 <= k - 1 < pieces:
            ring_relay(k - 1)
        if 0 <= k - 2 < pieces:
            ring_total(k - 2)
        if 0 <= k - 3 < pieces:
            line_middle(k - 3)
        if 0 <= k - 4 < pieces:
            line_total(k - 4)
    some_grads(3 * blocks)
    for k in range(pieces):
        arrived(mr.at[k, 1], mixed_out.at[:, back_cols(k, 1 - here.core)])
    for copy in plain:
        copy.wait_send()
    for cond, copy in guarded:
        @pl.when(cond)
        def _():
            copy.wait_send()


def expert_stage(x, cot, small, state, gate, up, down):
    tok_rows, width = x.shape
    hidden_dev, features = gate.shape
    pieces, wide = 4, 2 * features // (2 * RING * 2)
    vmem = pl.BlockSpec(memory_space=pltpu.VMEM)
    dma = pltpu.SemaphoreType.DMA
    f32, bf16 = jnp.float32, jnp.bfloat16
    full = (RING, tok_rows, features)
    acts = (RING, tok_rows, hidden_dev)
    block = (tok_rows, wide)
    return pl.pallas_call(
        expert_kernel,
        out_shape=[jax.ShapeDtypeStruct((hidden_dev, features), f32)] * 3 + [
            jax.ShapeDtypeStruct((tok_rows, features), bf16),
            jax.ShapeDtypeStruct((RING,) + small.shape, small.dtype),
            jax.ShapeDtypeStruct((RING,) + state.shape, state.dtype),
        ],
        in_specs=[vmem] * 7,
        out_specs=[vmem] * 6,
        scratch_shapes=[
            pltpu.VMEM(full, bf16), pltpu.VMEM(full, bf16),
            pltpu.VMEM(acts, f32), pltpu.VMEM(acts, f32),
            pltpu.VMEM(acts, bf16), pltpu.VMEM(acts, bf16), pltpu.VMEM(acts, bf16),
            pltpu.VMEM((pieces, RING) + block, bf16), pltpu.VMEM((pieces, RING) + block, bf16),
            pltpu.VMEM((pieces, RING) + block, bf16),
            pltpu.VMEM((pieces, 2, tok_rows // 2, wide), bf16),
            pltpu.VMEM((pieces, 2) + block, bf16),
            pltpu.VMEM((pieces,) + block, bf16), pltpu.VMEM((pieces,) + block, bf16),
            pltpu.VMEM((pieces, 2) + block, bf16),
            dma((2, 3)), dma((2, 3)),
            dma((2, 2, 5)), dma((2, 2, 3)),
            dma((2, 5, 6)), dma((2, 5, 6)),
            dma((2, 4, 5)), dma((2, 4, 5)),
            dma((pieces, 4)), dma((pieces, 4)),
            dma((pieces, 2)), dma((pieces, 2)),
            dma((pieces, 4)), dma((pieces, 4)),
            dma((pieces, 2)), dma((pieces, 2)),
            dma((pieces, 2)), dma((pieces, 2)),
        ],
        compiler_params=pltpu.CompilerParams(
            collective_id=0, has_side_effects=True, vmem_limit_bytes=60 << 20
        ),
        name="expert_stage",
    )(x, cot, small, state, gate, up, down)


def exchange_kernel(x_ref, out_ref, send_sem, recv_sem):
    here = Place()
    devices = (here.right, here.across, here.left)
    greet(devices)
    sends = []
    for step in (1, 3, 2):
        copy = remote(
            x_ref.at[here.at[step]], out_ref.at[here.sp],
            send_sem.at[step - 1], recv_sem.at[3 - step], devices[step - 1],
        )
        copy.start()
        sends.append(copy)
    out_ref[here.sp] = x_ref[here.sp]
    for step in (1, 2, 3):
        arrived(recv_sem.at[step - 1], out_ref.at[here.at[step]])
    for copy in sends:
        copy.wait_send()


def exchange(x, number):
    vmem = pl.BlockSpec(memory_space=pltpu.VMEM)
    dma = pltpu.SemaphoreType.DMA
    return pl.pallas_call(
        exchange_kernel,
        out_shape=jax.ShapeDtypeStruct(x.shape, x.dtype),
        in_specs=[vmem],
        out_specs=vmem,
        scratch_shapes=[dma((3,)), dma((3,))],
        compiler_params=pltpu.CompilerParams(collective_id=number, has_side_effects=True),
        name="exchange" + str(number),
    )(x)


def ring_local(
    layer_in, out_cot, route_ids, route_probs, group_prob, gate_weight, up_weight,
    down_weight, out_weight, query, key_in, value, decay_logit,
):
    tok_rows, local_cols = layer_in.shape
    experts_all = lax.axis_size("sp")
    here = lax.axis_index("sp")
    route_weight = group_prob[:, None] * route_probs / jnp.sum(route_probs, axis=1, keepdims=True)
    table = jnp.sum(
        jnp.where(
            route_ids[None] == jnp.arange(experts_all, dtype=jnp.int32)[:, None, None],
            route_weight[None],
            0.0,
        ),
        axis=2,
    )
    head_dev = query.shape[1] // DK

    def heads(tensor):
        return tensor.astype(jnp.float32).reshape(tok_rows, head_dev, -1).transpose(1, 0, 2)

    def flat(tensor):
        return tensor.transpose(1, 0, 2).reshape(tok_rows, -1)

    def product(spec, a, b):
        return jnp.einsum(spec, a, b, precision=highest)

    scaled_query = heads(query) * DK ** (-0.5)
    key_h, value_h, logit_h = heads(key_in), heads(value), heads(decay_logit)
    causal = jnp.tril(jnp.ones((tok_rows, tok_rows), dtype=bool))
    ones = causal.astype(jnp.float32)
    cumulative = product("cs,hsd->hcd", ones, jax.nn.log_sigmoid(logit_h) / decay_temp)
    span_log = cumulative[:, -1:, :]
    growth, shrink = jnp.exp(cumulative), jnp.exp(-cumulative)
    to_end = jnp.exp(span_log - cumulative)
    query_decayed, key_back, key_to_end = scaled_query * growth, key_h * shrink, key_h * to_end
    span_decay = jnp.exp(span_log[:, 0, :])
    span_state = product("hcd,hcv->hdv", key_to_end, value_h)
    lanes = -(-max(tok_rows, head_dev * DK) // 128) * 128
    small = jnp.zeros((8, lanes), jnp.float32)
    small = small.at[:experts_all, :tok_rows].set(table)
    small = small.at[experts_all, : head_dev * DK].set(span_decay.reshape(-1))
    gate_g, up_g, down_g, full_mixed, smalls, states = expert_stage(
        layer_in, out_cot, small, span_state.astype(jnp.bfloat16).reshape(head_dev * DK, DV),
        gate_weight[0], up_weight[0], down_weight[0],
    )
    decays = smalls[:, experts_all, : head_dev * DK].reshape(RING, head_dev, DK, 1)
    states = states.astype(jnp.float32).reshape(RING, head_dev, DK, DV)
    entry_state = jnp.zeros((head_dev, DK, DV), jnp.float32)
    for s in range(RING - 1):
        entry_state = jnp.where(s < here, entry_state * decays[s] + states[s], entry_state)
    span_end = span_decay[..., None] * entry_state + span_state
    scores = jnp.where(causal, product("hcd,hsd->hcs", query_decayed, key_back), 0.0)
    outputs = product("hcs,hsv->hcv", scores, value_h) + product(
        "hcd,hdv->hcv", query_decayed, entry_state
    )
    mixer_out = flat(outputs).astype(jnp.bfloat16)
    mixer_cot = jnp.dot(full_mixed, out_weight, preferred_element_type=jnp.float32)
    proj_parts = contract_rows(full_mixed, mixer_out).astype(jnp.bfloat16)
    proj_parts = exchange(proj_parts.reshape(RING, -1, proj_parts.shape[1]), 1)
    proj_grad = jnp.sum(proj_parts.astype(jnp.float32), axis=0)
    cot_h = heads(mixer_cot)
    span_future = product("hcd,hcv->hdv", query_decayed, cot_h)
    futures = exchange(
        jnp.broadcast_to(
            span_future.astype(jnp.bfloat16).reshape(1, head_dev * DK, DV), (RING, head_dev * DK, DV)
        ),
        2,
    )
    futures = futures.astype(jnp.float32).reshape(RING, head_dev, DK, DV)
    future_state = jnp.zeros((head_dev, DK, DV), jnp.float32)
    for s in range(RING - 1, 0, -1):
        future_state = jnp.where(s > here, future_state * decays[s] + futures[s], future_state)
    cot_values = jnp.where(causal, product("hcv,hsv->hcs", cot_h, value_h), 0.0)
    query_scaled_grad = growth * (
        product("hcv,hdv->hcd", cot_h, entry_state) + product("hcs,hsd->hcd", cot_values, key_back)
    )
    key_grad = shrink * product("hcs,hcd->hsd", cot_values, query_decayed) + to_end * product(
        "hsv,hdv->hsd", value_h, future_state
    )
    value_grad = product("hcs,hcv->hsv", scores, cot_h) + product(
        "hsd,hdv->hsv", key_to_end, future_state
    )
    decay_terms = scaled_query * query_scaled_grad - key_h * key_grad
    tail_sum = product("cs,hcd->hsd", ones, decay_terms)
    log_grad = tail_sum + jnp.sum(future_state * span_end, axis=2)[:, None, :]
    logit_grad = flat(log_grad * jax.nn.sigmoid(-logit_h) / decay_temp)
    return (
        gate_g[None], up_g[None], down_g[None], proj_grad,
        flat(query_scaled_grad * DK ** (-0.5)), flat(key_grad), flat(value_grad), logit_grad,
    )


def solution(mesh):
    in_specs = (
        P("sp", "tp"),
        P("sp", "tp"),
        P("sp", None),
        P("sp", None),
        P("sp"),
        P("sp", "tp", None),
        P("sp", "tp", None),
        P("sp", "tp", None),
        P(None, "tp"),
        P("sp", "tp"),
        P("sp", "tp"),
        P("sp", "tp"),
        P("sp", "tp"),
    )
    out_specs = (
        P("sp", "tp", None),
        P("sp", "tp", None),
        P("sp", "tp", None),
        P("sp", "tp"),
        P("sp", "tp"),
        P("sp", "tp"),
        P("sp", "tp"),
        P("sp", "tp"),
    )
    rows = 4 // mesh.shape["sp"]
    body = ring_local if rows * 4 == 4 and mesh.shape["tp"] == 8 else local
    return jax.shard_map(body, mesh=mesh, in_specs=in_specs, out_specs=out_specs, check_vma=False)
```

```python
import functools
import jax
import jax.numpy as jnp
from jax import lax
from jax.experimental import pallas as pl
from jax.experimental.pallas import tpu as pltpu
from jax.sharding import PartitionSpec as P

DK = 64
DV = 128
BLOCK = 64


decay_temp = 16.0
highest = lax.Precision.HIGH


def prefix(x, axis, join, neutral, backward):
    count = lax.axis_size(axis)
    place = lax.axis_index(axis)
    ahead = count - 1 - place if backward else place
    gathered = jax.tree.map(
        lambda a, kind: lax.all_gather(a.astype(kind), axis),
        x,
        jax.tree.map(lambda a: jnp.bfloat16 if a.dtype == jnp.float32 else a.dtype, x),
    )
    state = jax.tree.map(lambda a, e: jnp.zeros_like(a) + jnp.asarray(e, a.dtype), x, neutral)

    def one(step, state):
        source = count - 1 - step if backward else step
        return join(
            state,
            jax.tree.map(
                lambda a, own: lax.dynamic_index_in_dim(a, source, 0, False).astype(own.dtype),
                gathered,
                x,
            ),
        )

    return lax.fori_loop(0, ahead, one, state)


def combine_spans(earlier, later):
    return (earlier[0] * later[0], later[1] + later[0][..., None] * earlier[1])


def contract_rows(left_mat, right_mat):
    return lax.dot_general(
        left_mat, right_mat, (((0,), (0,)), ((), ())), preferred_element_type=jnp.float32
    )


def contract_cols(left_mat, right_mat):
    return lax.dot_general(
        left_mat, right_mat, (((1,), (1,)), ((), ())), preferred_element_type=jnp.float32
    )


def to_blocks(tensor, head_count):
    rows_here = tensor.shape[0]
    return (
        tensor.astype(jnp.float32)
        .reshape(rows_here // BLOCK, BLOCK, head_count, -1)
        .transpose(2, 0, 1, 3)
    )


def from_blocks(tensor):
    head_count, blocks, _, channels = tensor.shape
    return tensor.transpose(1, 2, 0, 3).reshape(blocks * BLOCK, head_count * channels)


def expert_pass(rows_x, rows_cot, gate_mat, up_mat, down_mat):
    full_x, full_cot = (
        lax.all_gather(rows_x, "tp", axis=1, tiled=True),
        lax.all_gather(rows_cot, "tp", axis=1, tiled=True),
    )
    gate_pre = contract_cols(full_x, gate_mat)
    up_pre = contract_cols(full_x, up_mat)
    sigmoid_gate = jax.nn.sigmoid(gate_pre)
    active = gate_pre * sigmoid_gate
    hidden = (active * up_pre).astype(jnp.bfloat16)
    hidden_cot = contract_cols(full_cot, down_mat)
    up_cot = (hidden_cot * active).astype(jnp.bfloat16)
    gate_cot = (
        hidden_cot * up_pre * sigmoid_gate * (1.0 + gate_pre * (1.0 - sigmoid_gate))
    ).astype(jnp.bfloat16)
    down_g = contract_rows(hidden, full_cot)
    gate_g = contract_rows(gate_cot, full_x)
    up_g = contract_rows(up_cot, full_x)
    dims = (((0,), (1,)), ((), ()))
    first_part = lax.dot_general(gate_mat, gate_cot, dims, preferred_element_type=jnp.float32)
    back_terms = lax.psum_scatter(
        (
            first_part + lax.dot_general(up_mat, up_cot, dims, preferred_element_type=jnp.float32)
        ).astype(jnp.bfloat16),
        "tp",
        scatter_dimension=0,
        tiled=True,
    ).astype(jnp.float32)
    return (gate_g, up_g, down_g, back_terms)


def local(
    layer_in,
    out_cot,
    route_ids,
    route_probs,
    group_prob,
    gate_weight,
    up_weight,
    down_weight,
    out_weight,
    query,
    key_in,
    value,
    decay_logit,
):
    tok_rows = layer_in.shape[0]
    local_cols = layer_in.shape[1]
    experts_all = lax.axis_size("sp")
    capacity = 4 * tok_rows // experts_all
    route_weight = group_prob[:, None] * route_probs / jnp.sum(route_probs, axis=1, keepdims=True)
    chosen = (route_ids[:, :, None] == jnp.arange(experts_all, dtype=jnp.int32)).astype(jnp.int32)
    running = jnp.cumsum(chosen.reshape(2 * tok_rows, experts_all), axis=0).reshape(
        tok_rows, 2, experts_all
    )
    position = jnp.sum((running - 1) * chosen, axis=2)
    slot_ids = route_ids * capacity + position
    matches = (
        slot_ids[None, :, :] == jnp.arange(experts_all * capacity, dtype=jnp.int32)[:, None, None]
    )
    select_x = jnp.any(matches, axis=2).astype(jnp.float32)
    select_cot = jnp.sum(jnp.where(matches, route_weight[None], 0.0), axis=2)
    send_x = jnp.dot(
        select_x.astype(jnp.bfloat16), layer_in, preferred_element_type=jnp.float32
    ).astype(jnp.bfloat16)
    send_cot = jnp.dot(select_cot, out_cot.astype(jnp.float32), precision=highest).astype(
        jnp.bfloat16
    )
    send_x = send_x.reshape(experts_all, capacity, local_cols)
    send_cot = send_cot.reshape(experts_all, capacity, local_cols)
    recv_x, recv_cot = (
        lax.all_to_all(send_x, "sp", split_axis=0, concat_axis=0, tiled=True),
        lax.all_to_all(send_cot, "sp", split_axis=0, concat_axis=0, tiled=True),
    )
    head_dev = query.shape[1] // DK
    scaled_query = to_blocks(query, head_dev) * DK ** (-0.5)
    key_blk = to_blocks(key_in, head_dev)
    value_blk = to_blocks(value, head_dev)
    logit_blk = to_blocks(decay_logit, head_dev)
    cumulative = jnp.cumsum(jax.nn.log_sigmoid(logit_blk) / decay_temp, axis=2)
    span_log = cumulative[:, :, -1:, :]
    growth = jnp.exp(cumulative)
    shrink = jnp.exp(-cumulative)
    to_end = jnp.exp(span_log - cumulative)
    query_decayed = scaled_query * growth
    key_back = key_blk * shrink
    key_to_end = key_blk * to_end
    causal = jnp.tril(jnp.ones((BLOCK, BLOCK), dtype=bool))
    scores = jnp.where(
        causal, jnp.einsum("hncd,hnsd->hncs", query_decayed, key_back, precision=highest), 0.0
    )
    within = jnp.einsum("hncs,hnsv->hncv", scores, value_blk, precision=highest)
    block_decay = jnp.moveaxis(jnp.exp(span_log[:, :, 0, :]), 1, 0)
    block_update = jnp.moveaxis(
        jnp.einsum("hncd,hncv->hndv", key_to_end, value_blk, precision=highest), 1, 0
    )
    identity_pair = (
        jnp.ones((head_dev, DK), jnp.float32),
        jnp.zeros((head_dev, DK, DV), jnp.float32),
    )

    def advance(carry_pair, inputs):
        return (combine_spans(carry_pair, inputs), carry_pair)

    span_total, before_pairs = lax.scan(advance, identity_pair, (block_decay, block_update))
    entry_pair = prefix(span_total, "sp", combine_spans, identity_pair, False)
    entry_state = entry_pair[1]
    decay_before = jnp.moveaxis(before_pairs[0], 0, 1)
    block_state = decay_before[..., None] * entry_state[:, None] + jnp.moveaxis(
        before_pairs[1], 0, 1
    )
    span_end = span_total[0][..., None] * entry_state + span_total[1]
    outputs = within + jnp.einsum("hncd,hndv->hncv", query_decayed, block_state, precision=highest)
    mixer_out = from_blocks(outputs).astype(jnp.bfloat16)
    gate_mat, up_mat, down_mat = (gate_weight[0], up_weight[0], down_weight[0])
    gate_g, up_g, down_g, back_flat = expert_pass(
        recv_x.reshape(-1, local_cols), recv_cot.reshape(-1, local_cols), gate_mat, up_mat, down_mat
    )
    back_terms = back_flat.reshape(local_cols, experts_all, capacity)
    returned = lax.all_to_all(
        back_terms.astype(jnp.bfloat16), "sp", split_axis=1, concat_axis=1, tiled=True
    ).astype(back_terms.dtype)
    returned = returned.reshape(local_cols, experts_all * capacity)
    routed_sum = lax.dot_general(
        select_x,
        returned,
        (((0,), (1,)), ((), ())),
        precision=highest,
        preferred_element_type=jnp.float32,
    )
    mixed_cot = (out_cot.astype(jnp.float32) + routed_sum).astype(jnp.bfloat16)
    full_cot = lax.all_gather(mixed_cot, "tp", axis=1, tiled=True)
    mixer_cot = jnp.dot(full_cot, out_weight, preferred_element_type=jnp.float32)
    proj_grad = lax.psum_scatter(
        contract_rows(full_cot, mixer_out).astype(jnp.bfloat16),
        "sp",
        scatter_dimension=0,
        tiled=True,
    ).astype(jnp.float32)
    cot_blk = to_blocks(mixer_cot, head_dev)
    block_future = jnp.moveaxis(
        jnp.einsum("hncd,hncv->hndv", query_decayed, cot_blk, precision=highest), 1, 0
    )

    def retreat(carry_pair, inputs):
        return (combine_spans(carry_pair, inputs), carry_pair)

    span_back, after_pairs = lax.scan(
        retreat, identity_pair, (block_decay, block_future), reverse=True
    )
    beyond_pair = prefix(span_back, "sp", combine_spans, identity_pair, True)
    future_state = beyond_pair[1]
    decay_after = jnp.moveaxis(after_pairs[0], 0, 1)
    block_future_state = decay_after[..., None] * future_state[:, None] + jnp.moveaxis(
        after_pairs[1], 0, 1
    )
    cot_values = jnp.where(
        causal, jnp.einsum("hncv,hnsv->hncs", cot_blk, value_blk, precision=highest), 0.0
    )
    query_scaled_grad = growth * (
        jnp.einsum("hncv,hndv->hncd", cot_blk, block_state, precision=highest)
        + jnp.einsum("hncs,hnsd->hncd", cot_values, key_back, precision=highest)
    )
    key_part = shrink * jnp.einsum("hncs,hncd->hnsd", cot_values, query_decayed, precision=highest)
    key_grad = key_part + to_end * jnp.einsum(
        "hnsv,hndv->hnsd", value_blk, block_future_state, precision=highest
    )
    value_grad = jnp.einsum("hncs,hncv->hnsv", scores, cot_blk, precision=highest) + jnp.einsum(
        "hnsd,hndv->hnsv", key_to_end, block_future_state, precision=highest
    )
    decay_terms = (scaled_query * query_scaled_grad - key_blk * key_grad).reshape(
        head_dev, tok_rows, DK
    )
    tail_sum = jnp.flip(jnp.cumsum(jnp.flip(decay_terms, 1), axis=1), 1)
    beyond_term = jnp.sum(future_state * span_end, axis=2)
    log_grad = tail_sum + beyond_term[:, None, :]
    logit_flat = logit_blk.reshape(head_dev, tok_rows, DK)
    logit_grad = (
        (log_grad * jax.nn.sigmoid(-logit_flat) / decay_temp)
        .transpose(1, 0, 2)
        .reshape(tok_rows, head_dev * DK)
    )
    query_grad = from_blocks(query_scaled_grad * DK ** (-0.5))
    return (
        gate_g[None],
        up_g[None],
        down_g[None],
        proj_grad,
        query_grad,
        from_blocks(key_grad),
        from_blocks(value_grad),
        logit_grad,
    )


RING = 4
EXPERT_CUT = 5
PIECES = 8
GATHER_ORDER = (
    ("rs", 1, 4),
    ("rs", 0, 4),
    ("zs", 0, 0),
    ("zs", 1, 0),
    ("rs", 0, 0),
    ("rf", 0, 4, 1),
    ("rf", 0, 4, 0),
    ("prep",),
    ("rf", 1, 4, 1),
    ("rf", 1, 4, 0),
    ("zr", 0, 0, 1),
    ("rs", 1, 0),
    ("zr", 0, 0, 2),
    ("zr", 1, 0, 1),
    ("rd", 0, 4),
    ("zr", 0, 0, 3),
    ("mixf",),
    ("rd", 1, 4),
    ("rf", 0, 1, 1),
    ("fx", 0),
    ("rf", 0, 1, 0),
    ("rf", 0, 0, 1),
    ("zr", 0, 1, 2),
    ("rf", 0, 2, 1),
    ("rf", 0, 0, 0),
    ("zr", 0, 1, 1),
    ("rf", 0, 2, 0),
    ("zr", 1, 0, 2),
    ("rf", 0, 3, 1),
    ("rf", 0, 3, 0),
    ("zr", 0, 1, 3),
    ("rf", 1, 0, 1),
    ("rf", 1, 0, 0),
    ("rf", 1, 1, 1),
    ("rd", 0, 1),
    ("zr", 1, 1, 1),
    ("zr", 1, 0, 3),
    ("rd", 0, 2),
    ("fx", 4),
    ("zr", 1, 1, 2),
    ("rf", 1, 1, 0),
    ("rf", 1, 2, 0),
    ("rf", 1, 2, 1),
    ("rd", 0, 0),
    ("sy", 0),
    ("rd", 0, 3),
    ("zr", 1, 1, 3),
    ("rd", 1, 0),
    ("rf", 1, 3, 1),
    ("rf", 1, 3, 0),
    ("fx", 1),
    ("rd", 1, 1),
    ("fx", 2),
    ("rd", 1, 2),
    ("sy", 4),
    ("rd", 1, 3),
    ("fx", 3),
    ("sy", 1),
    ("sy", 2),
    ("sy", 3),
)
REDUCE_ORDER = (
    ("pt", 0),
    ("pt", 1),
    ("op", 0),
    ("g", 10),
    ("pt", 2),
    ("op", 1),
    ("g", 6),
    ("pt", 3),
    ("rl", 1, 1),
    ("rl", 1, 0),
    ("rl", 0, 0),
    ("rl", 0, 1),
    ("op", 2),
    ("g", 8),
    ("to", 1),
    ("rl", 2, 0),
    ("rl", 3, 1),
    ("rl", 4, 0),
    ("rl", 3, 0),
    ("g", 7),
    ("rl", 2, 1),
    ("rl", 4, 1),
    ("op", 3),
    ("to", 0),
    ("rl", 5, 1),
    ("mi", 1),
    ("to", 2),
    ("to", 3),
    ("to", 4),
    ("mi", 0),
    ("rl", 5, 0),
    ("rl", 6, 0),
    ("rl", 6, 1),
    ("lt", 1),
    ("rl", 7, 1),
    ("rl", 7, 0),
    ("mi", 2),
    ("mi", 3),
    ("to", 5),
    ("g", 0),
    ("to", 6),
    ("to", 7),
    ("lt", 0),
    ("mi", 4),
    ("lt", 2),
    ("g", 11),
    ("gd", 0),
    ("lt", 3),
    ("mi", 5),
    ("gd", 1),
    ("pj", 0),
    ("gd", 2),
    ("g", 5),
    ("lt", 4),
    ("gd", 3),
    ("mi", 6),
    ("g", 3),
    ("mi", 7),
    ("pj", 1),
    ("lt", 5),
    ("gd", 4),
    ("g", 1),
    ("lt", 6),
    ("gd", 5),
    ("g", 4),
    ("pj", 2),
    ("lt", 7),
    ("gd", 6),
    ("g", 2),
    ("gd", 7),
    ("mb",),
    ("pj", 3),
    ("mb2",),
    ("g", 9),
    ("mb3",),
    ("mf",),
)


def ring_place(index):
    return index + (index // 2) * (1 - 2 * (index % 2))


def remote(source, target, send_sem, recv_sem, device):
    return pltpu.make_async_remote_copy(
        src_ref=source,
        dst_ref=target,
        send_sem=send_sem,
        recv_sem=recv_sem,
        device_id=device,
        device_id_type=pl.DeviceIdType.MESH,
    )


def greet(devices):
    barrier = pltpu.get_barrier_semaphore()
    for device in devices:
        pl.semaphore_signal(
            barrier, inc=1, device_id=device, device_id_type=pl.DeviceIdType.MESH
        )
    pl.semaphore_wait(barrier, len(devices))


def arrived(sem, region):
    pltpu.make_async_copy(region, region, sem).wait()


class Place:
    def __init__(self):
        self.sp, self.tp = lax.axis_index("sp"), lax.axis_index("tp")
        self.z, self.core = self.tp // 2, self.tp % 2
        ring = ring_place(self.sp)
        self.at = [ring_place((ring + step) % RING) for step in range(RING)]
        self.right, self.across, self.left = [(self.at[s], self.tp) for s in (1, 2, 3)]
        self.pair = (self.sp, 2 * self.z + 1 - self.core)
        self.near = (self.sp, 2 * (self.z + 1 - 2 * (self.z % 2)) + self.core)
        self.far = (self.sp, 2 * (RING - 1 - self.z) + self.core)
        upper = self.z // 2
        folded = self.z + upper * (RING - 1 - 2 * self.z)
        self.inner = folded == 1
        self.end = folded == 0
        order = [folded, 1 - folded, 2, 3]
        self.slot = [o + upper * (RING - 1 - 2 * o) for o in order]


def layer_kernel(
    x_ref, cot_ref, small_ref, gate_ref, up_ref, down_ref, out_ref,
    query_ref, key_ref, value_ref, logit_ref,
    gate_out, up_out, down_out, proj_out, query_out, key_out, value_out, logit_out,
    mixed, small_buf, small_out, state_buf, state_out, future_buf, future_out,
    decayed, key_back, key_end, state_own, entry, span_end, scores, mixer_out, mixer_cot,
    proj_to, proj_from, summed, terms, weights,
    x_all, cot_all, gate_pre, up_pre, hidden, gate_cot, up_cot,
    pair_to, pair_from, parts, first_in, second_in, total, half_total, z_in,
    tiny_send, tiny_recv, zs, zr, ps, pr, qs, qr,
    fs, fr, js, jr, bs, br, r1s, r1r, r2s, r2r, zts, ztr, ms, mr,
):
    here = Place()
    tok_rows, width = x_ref.shape
    lead = tok_rows * 4 // EXPERT_CUT
    tail = tok_rows - lead
    ins, alls = (x_ref, cot_ref), (x_all, cot_all)
    greet([here.right, here.across, here.left, here.near, here.far, here.pair])
    plain, guarded = [], []

    def go(source, target, send_sem, recv_sem, device):
        copy = remote(source, target, send_sem, recv_sem, device)
        copy.start()
        plain.append(copy)

    def go_if(cond, source, target, send_sem, recv_sem, device):
        copy = remote(source, target, send_sem, recv_sem, device)

        @pl.when(cond)
        def _():
            copy.start()

        guarded.append((cond, copy))

    def cols(slot, core):
        return pl.ds(pl.multiple_of((2 * here.slot[slot] + core) * width, width), width)

    def piece(a, part, slot, core=None):
        core = here.core if core is None else core
        if part == 0:
            return alls[a].at[here.sp, pl.ds(0, lead), cols(slot, core)]
        return alls[a].at[:, pl.ds(lead, tail), cols(slot, core)]

    def own_rows(a, start, count):
        return ins[a].at[pl.ds(start, count), :]

    def z_start(a, part):
        source = own_rows(a, 0, lead) if part == 0 else piece(a, 1, 0)
        target = piece(a, part, 0)
        go(source, target, zs.at[a, part, 0], zr.at[a, part, 0], here.near)
        go_if(here.inner, source, target, zs.at[a, part, 1], zr.at[a, part, 1], here.far)

    def z_relay(a, part, slot):
        region = piece(a, part, slot)
        arrived(zr.at[a, part, slot - 1], region)
        if slot == 1:
            go_if(here.inner, region, region, zs.at[a, part, 2], zr.at[a, part, 2], here.far)
        else:
            go_if(
                here.inner, region, region, zs.at[a, part, slot + 1], zr.at[a, part, slot - 1],
                here.near,
            )
        if part == 0:
            pair_send(a, slot, 0)
            ring_send(a, (slot, 0))
        else:
            go(region, region, qs.at[a, slot, 4], qr.at[a, slot, 4], here.pair)

    def bounds(part, h):
        start, count = (0, lead) if part == 0 else (lead, tail)
        return start + h * (count // 2), count // 2

    def ring_region(a, unit, step, h):
        slot, part = unit
        start, count = bounds(part, h)
        return alls[a].at[here.at[step], pl.ds(start, count), cols(slot, here.core)]

    def number(unit):
        return unit[0] + 4 * unit[1]

    def ring_send(a, unit):
        slot, part = unit
        n = number(unit)
        for i, (h, device) in enumerate(
            ((0, here.right), (1, here.right), (0, here.left), (1, here.left))
        ):
            start, count = bounds(part, h)
            source = own_rows(a, start, count) if slot == 0 else ring_region(a, unit, 0, h)
            copy = remote(source, ring_region(a, unit, 0, h), ps.at[a, n, i], pr.at[a, n, i], device)
            plain.append(copy)
        right0, right1, left0, left1 = plain[-4:]
        for copy in (right0, left1, right1, left0):
            copy.start()

    def ring_forward(a, unit, h):
        n = number(unit)
        region = ring_region(a, unit, (3, 1)[h], h)
        arrived(pr.at[a, n, 3 * h], region)
        go(region, region, ps.at[a, n, 4 + h], pr.at[a, n, 4 + h], (here.right, here.left)[h])

    def ring_finish(a, unit):
        n = number(unit)
        arrived(pr.at[a, n, 1], ring_region(a, unit, 3, 1))
        arrived(pr.at[a, n, 2], ring_region(a, unit, 1, 0))
        arrived(pr.at[a, n, 4], ring_region(a, unit, 2, 0))
        arrived(pr.at[a, n, 5], ring_region(a, unit, 2, 1))
        if unit[1] == 0:
            for step in (1, 3, 2):
                pair_send(a, unit[0], step)
        else:
            z_start(a, 1)
            region = piece(a, 1, 0)
            go(region, region, qs.at[a, 0, 4], qr.at[a, 0, 4], here.pair)

    def pair_region(a, slot, step, core):
        return alls[a].at[here.at[step], pl.ds(0, lead), cols(slot, core)]

    def pair_send(a, slot, step):
        region = pair_region(a, slot, step, here.core)
        source = own_rows(a, 0, lead) if slot == 0 and step == 0 else region
        go(source, region, qs.at[a, slot, step], qr.at[a, slot, step], here.pair)

    def pair_wait(a, step):
        for slot in range(RING):
            if step < 4:
                arrived(qr.at[a, slot, step], pair_region(a, slot, step, 1 - here.core))
            else:
                arrived(qr.at[a, slot, 4], piece(a, 1, slot, 1 - here.core))

    bf16, f32 = jnp.bfloat16, jnp.float32
    key_cols = query_ref.shape[1]
    heads = key_cols // DK
    lane = lax.broadcasted_iota(jnp.int32, (1, key_cols), 1) // DK
    row = lax.broadcasted_iota(jnp.int32, (key_cols, 1), 0) // DK

    def dot(left, right, left_dim=1, right_dim=0, precision=None):
        return lax.dot_general(
            left, right, (((left_dim,), (right_dim,)), ((), ())),
            precision=precision, preferred_element_type=f32,
        )

    def two(value):
        high = value.astype(bf16)
        return high, (value - high.astype(f32)).astype(bf16)

    def triangle():
        return lax.broadcasted_iota(jnp.int32, (tok_rows, tok_rows), 0) >= (
            lax.broadcasted_iota(jnp.int32, (tok_rows, tok_rows), 1)
        )

    def only(value, h):
        return jnp.where(lane == h, value, jnp.zeros_like(value))

    def join(parts_of, which):
        joined = parts_of[0]
        for h in range(1, heads):
            joined = jnp.where(which == h, parts_of[h], joined)
        return joined

    def head_cols(h):
        return pl.ds(h * DV, DV)

    def log_decay(logit):
        return -(jnp.maximum(-logit, 0.0) + jnp.log(1.0 + jnp.exp(-jnp.abs(logit)))) / decay_temp

    def column(s):
        pick = (
            lax.broadcasted_iota(jnp.int32, (small_buf.shape[0], DV), 0) == RING
        ).astype(f32)
        return dot(
            small_out[s, :, pl.ds(0, key_cols)], pick, 0, 0, lax.Precision.HIGHEST
        )

    def mix_prepare():
        ones = triangle().astype(bf16)
        high, low = two(log_decay(logit_ref[...].astype(f32)))
        cumulative = dot(ones, high) + dot(ones, low)
        summed[...] = cumulative
        last = cumulative[tok_rows - 1 : tok_rows, :]
        keys = key_ref[...].astype(f32)
        decayed[...] = (
            query_ref[...].astype(f32) * DK ** (-0.5) * jnp.exp(cumulative)
        ).astype(bf16)
        key_back[...] = (keys * jnp.exp(-cumulative)).astype(bf16)
        ends = (keys * jnp.exp(last - cumulative)).astype(bf16)
        key_end[...] = ends
        state = join([dot(ends, value_ref[:, head_cols(h)], 0, 0) for h in range(heads)], row)
        state_own[...] = state
        state_buf[...] = state.astype(bf16)
        small_buf[:, pl.ds(0, tok_rows)] = small_ref[...]
        small_buf[RING : RING + 1, pl.ds(0, key_cols)] = jnp.exp(last)
        small_out[here.sp] = small_buf[...]
        state_out[here.sp] = state_buf[...]
        for i, (buf, out) in enumerate(((small_buf, small_out), (state_buf, state_out))):
            for step, device in ((1, here.right), (3, here.left), (2, here.across)):
                go(
                    buf, out.at[here.sp], tiny_send.at[i, step - 1], tiny_recv.at[i, 3 - step],
                    device,
                )

    def mix_forward():
        for step in (1, 2, 3):
            arrived(tiny_recv.at[0, step - 1], small_out.at[here.at[step]])
            arrived(tiny_recv.at[1, step - 1], state_out.at[here.at[step]])
        state = jnp.zeros((key_cols, DV), f32)
        for s in range(RING - 1):
            later = state * column(s) + state_out[s].astype(f32)
            state = jnp.where(here.sp > s, later, state)
        entry[...] = state.astype(bf16)
        mine = (
            lax.broadcasted_iota(jnp.int32, (small_buf.shape[0], 128), 0) == here.sp
        ).astype(f32)
        for s in range(RING):
            weights[s] = dot(small_out[s], mine, 0, 0, lax.Precision.HIGHEST)[:tok_rows]
        span_end[...] = state * column(here.sp) + state_own[...]
        keep = triangle()
        for h in range(heads):
            mine = only(decayed[...], h)
            score = jnp.where(keep, dot(mine, key_back[...], 1, 1), 0.0).astype(bf16)
            scores[h] = score
            mixer_out[:, head_cols(h)] = (
                dot(score, value_ref[:, head_cols(h)]) + dot(mine, entry[...])
            ).astype(bf16)

    def mix_backward():
        cot = [mixer_cot[:, head_cols(h)].astype(bf16) for h in range(heads)]
        future = join([dot(decayed[...], cot[h], 0, 0) for h in range(heads)], row)
        future_buf[...] = future.astype(bf16)
        for step, device in ((1, here.right), (3, here.left), (2, here.across)):
            go(
                future_buf, future_out.at[here.sp], fs.at[step - 1], fr.at[3 - step], device
            )

    held = {}

    def mix_inner():
        keep = triangle()
        cot = [mixer_cot[:, head_cols(h)].astype(bf16) for h in range(heads)]
        pairs = [
            jnp.where(keep, dot(cot[h], value_ref[:, head_cols(h)], 1, 1), 0.0).astype(bf16)
            for h in range(heads)
        ]
        inner = join(
            [dot(cot[h], entry[...], 1, 1) + dot(pairs[h], key_back[...]) for h in range(heads)],
            lane,
        )
        key_inner = join([dot(pairs[h], decayed[...], 0, 0) for h in range(heads)], lane)
        query_out[...] = jnp.exp(summed[...]) * inner * DK ** (-0.5)
        key_out[...] = jnp.exp(-summed[...]) * key_inner
        terms[...] = (
            decayed[...].astype(f32) * inner - key_back[...].astype(f32) * key_inner
        )
        for h in range(heads):
            value_out[:, head_cols(h)] = dot(scores[h], cot[h], 0, 0)

    def mix_outer():
        for step in (1, 2, 3):
            arrived(fr.at[step - 1], future_out.at[here.at[step]])
        state = jnp.zeros((key_cols, DV), f32)
        for s in range(RING - 1, 0, -1):
            earlier = state * column(s) + future_out[s].astype(f32)
            state = jnp.where(here.sp < s, earlier, state)
        ahead = state.astype(bf16)
        key_outer = join(
            [dot(value_ref[:, head_cols(h)], ahead, 1, 1) for h in range(heads)], lane
        )
        last = summed[tok_rows - 1 : tok_rows, :]
        key_out[...] += jnp.exp(last - summed[...]) * key_outer
        for h in range(heads):
            value_out[:, head_cols(h)] += dot(only(key_end[...], h), ahead)
        high, low = two(terms[...] - key_end[...].astype(f32) * key_outer)
        ones = triangle().astype(bf16)
        tail_sum = dot(ones, high, 0, 0) + dot(ones, low, 0, 0)
        beyond = dot(
            jnp.ones((8, DV), f32), state * span_end[...], 1, 1, lax.Precision.HIGHEST
        )[0:1, :]
        logit_out[...] = (tail_sum + beyond) / (
            decay_temp * (1.0 + jnp.exp(logit_ref[...].astype(f32)))
        )

    def mix_finish():
        for m in range(RING):
            result = proj_to[m, here.sp].astype(f32)
            for step in (1, 3, 2):
                arrived(jr.at[m, step - 1], proj_from.at[m, here.at[step]])
                result = result + proj_from[m, here.at[step]].astype(f32)
            proj_out[pl.ds(m * atom, atom), :] = result

    def block_of(ref, s):
        if s is None:
            return ref[:, pl.ds(lead, tail), :].reshape(RING * tail, ref.shape[2])
        return ref[s, pl.ds(0, lead), :]

    def keep_block(ref, s, value):
        if s is None:
            ref[:, pl.ds(lead, tail), :] = value.reshape(RING, tail, ref.shape[2])
        else:
            ref[s, pl.ds(0, lead), :] = value

    def forward_rows(s):
        block = block_of(x_all, s)
        keep_block(gate_pre, s, contract_cols(block, gate_ref[...]))
        keep_block(up_pre, s, contract_cols(block, up_ref[...]))

    def second_rows(s):
        weight = jnp.concatenate([block_of(weights, s)] * (width // 128), axis=1)
        hidden_cot = contract_cols(block_of(cot_all, s), down_ref[...]) * weight
        gp, upp = block_of(gate_pre, s), block_of(up_pre, s)
        sig = 1.0 / (1.0 + jnp.exp(-gp))
        active = gp * sig
        keep_block(hidden, s, (active * upp * weight).astype(jnp.bfloat16))
        keep_block(up_cot, s, (hidden_cot * active).astype(jnp.bfloat16))
        keep_block(
            gate_cot, s,
            (hidden_cot * upp * sig * (1.0 + gp * (1.0 - sig))).astype(jnp.bfloat16),
        )

    def rows_of(a, step, work):
        pair_wait(a, step)
        work(here.at[step] if step < RING else None)

    def own_start(a):
        ring_send(a, (0, 0))
        pair_send(a, 0, 0)

    gather_steps = {
        "zs": z_start,
        "rs": lambda a, n: own_start(a) if n == 0 else ring_send(a, (0, 1)),
        "zr": z_relay,
        "rf": lambda a, n, h: ring_forward(a, (n % 4, n // 4), h),
        "rd": lambda a, n: ring_finish(a, (n % 4, n // 4)),
        "prep": mix_prepare,
        "mixf": mix_forward,
        "fx": lambda i: rows_of(0, i, forward_rows),
        "sy": lambda i: rows_of(1, i, second_rows),
    }
    for a in range(2):
        alls[a][here.sp, :, cols(0, here.core)] = ins[a][...]
    for name, *rest in GATHER_ORDER:
        gather_steps[name](*rest)

    pieces, wide = parts.shape[0], parts.shape[3]
    split = tok_rows // 2
    span = gate_ref.shape[1] // RING
    atom = span // RING
    per = 2 * atom // wide

    def atoms(k, core):
        for i in range(wide // atom):
            target = 2 * core + (k % per) + i
            yield pl.ds(pl.multiple_of(target * span + (k // per) * atom, atom), atom)

    def columns(ref, k, core):
        return jnp.concatenate([ref[:, c] for c in atoms(k, core)], axis=1)

    top, bottom = pl.ds(0, split), pl.ds(split, split)

    def partial(m, core):
        rows = RING * tok_rows
        total_of = [
            jnp.dot(
                cot[...].reshape(rows, width),
                jnp.concatenate([columns(ref, m * per + i, core) for i in range(per)], axis=1),
                preferred_element_type=jnp.float32,
            )
            for cot, ref in ((gate_cot, gate_ref), (up_cot, up_ref))
        ]
        both = total_of[0] + total_of[1]
        for i in range(per):
            part = both[:, i * wide : (i + 1) * wide]
            yield m * per + i, part.reshape(RING, tok_rows, wide)

    def pair_part(m):
        for k, part in partial(m, 1 - here.core):
            pair_to[k] = part.astype(jnp.bfloat16)
            go(pair_to.at[k], pair_from.at[k], bs.at[k], br.at[k], here.pair)

    def own_part(m):
        for k, part in partial(m, here.core):
            arrived(br.at[k], pair_from.at[k])
            parts[k] = (part + pair_from[k].astype(jnp.float32)).astype(jnp.bfloat16)
            right, across, left = [parts.at[k, here.at[i]] for i in (1, 2, 3)]
            go(across.at[top], first_in.at[k, 0], r1s.at[k, 0], r1r.at[k, 0], here.right)
            go(across.at[bottom], first_in.at[k, 1], r1s.at[k, 1], r1r.at[k, 1], here.left)
            go(
                right.at[bottom], second_in.at[k, 0, bottom], r2s.at[k, 0], r2r.at[k, 0],
                here.right,
            )
            go(left.at[top], second_in.at[k, 1, top], r2s.at[k, 1], r2r.at[k, 1], here.left)

    def add_to(ref, other):
        ref[...] = (ref[...].astype(jnp.float32) + other.astype(jnp.float32)).astype(jnp.bfloat16)

    def ring_relay(k, h):
        step, rows, device = ((1, top, here.right), (3, bottom, here.left))[h]
        arrived(r1r.at[k, h], first_in.at[k, h])
        mine = parts.at[k, here.at[step]].at[rows]
        add_to(mine, first_in[k, h])
        go(
            mine, second_in.at[k, h, rows],
            r2s.at[k, 2 + h], r2r.at[k, 2 + h], device,
        )

    def ring_total(k):
        arrived(r2r.at[k, 0], second_in.at[k, 0, bottom])
        arrived(r2r.at[k, 1], second_in.at[k, 1, top])
        arrived(r2r.at[k, 2], second_in.at[k, 0, top])
        arrived(r2r.at[k, 3], second_in.at[k, 1, bottom])
        total[k] = (
            parts[k, here.sp].astype(jnp.float32)
            + second_in[k, 0].astype(jnp.float32)
            + second_in[k, 1].astype(jnp.float32)
        ).astype(jnp.bfloat16)
        go_if(here.end, total.at[k], z_in.at[k, 0], zts.at[k, 0], ztr.at[k, 0], here.near)

    def line_middle(k):
        copy = remote(half_total.at[k], z_in.at[k, 1], zts.at[k, 1], ztr.at[k, 1], here.far)

        @pl.when(here.inner)
        def _():
            arrived(ztr.at[k, 0], z_in.at[k, 0])
            half_total[k] = (
                total[k].astype(jnp.float32) + z_in[k, 0].astype(jnp.float32)
            ).astype(jnp.bfloat16)
            copy.start()

        guarded.append((here.inner, copy))

    def line_total(k):
        region = mixed.at[k, here.core]
        copy = remote(region, region, ms.at[k, 0], mr.at[k, 0], here.near)

        @pl.when(here.inner)
        def _():
            arrived(ztr.at[k, 1], z_in.at[k, 1])
            mixed[k, here.core] = (
                columns(cot_all.at[here.sp], k, here.core).astype(jnp.float32)
                + (half_total[k].astype(jnp.float32) + z_in[k, 1].astype(jnp.float32))
            ).astype(jnp.bfloat16)
            copy.start()

        guarded.append((here.inner, copy))

        @pl.when(here.end)
        def _():
            arrived(mr.at[k, 0], region)

        go(region, region, ms.at[k, 1], mr.at[k, 1], here.pair)

    features = gate_ref.shape[1]
    block_cols = 2 * width

    def weight_grad(n):
        which, j = n % 3, n // 3
        left, right, out = (
            (gate_cot, x_all, gate_out), (up_cot, x_all, up_out), (hidden, cot_all, down_out)
        )[which]
        c = pl.ds(j * block_cols, block_cols)
        rows = RING * tok_rows
        out[:, c] = contract_rows(
            left[...].reshape(rows, width), right[:, :, c].reshape(rows, block_cols)
        )

    def mixed_group(m):
        return jnp.concatenate(
            [mixed[m * per + i, core] for core in range(2) for i in range(per)], axis=1
        )

    def group_done(k):
        arrived(mr.at[k, 1], mixed.at[k, 1 - here.core])
        if (k + 1) % per:
            return
        m = k // per
        group = mixed_group(m)
        weight = jnp.concatenate(
            [out_ref[pl.ds(d * span + m * atom, atom), :] for d in range(RING)], axis=0
        )
        term = dot(group, weight)
        mixer_cot[...] = term if m == 0 else mixer_cot[...] + term

    def group_proj(m):
        group = mixed_group(m)
        block = dot(group, mixer_out[...], 0, 0).astype(bf16)
        for d in range(RING):
            proj_to[m, d] = block[d * atom : (d + 1) * atom, :]
        for step, device in ((1, here.right), (3, here.left), (2, here.across)):
            go(
                proj_to.at[m, here.at[step]], proj_from.at[m, here.sp],
                js.at[m, step - 1], jr.at[m, 3 - step], device,
            )

    reduce_steps = {
        "pt": pair_part,
        "op": own_part,
        "g": weight_grad,
        "rl": ring_relay,
        "to": ring_total,
        "mi": line_middle,
        "lt": line_total,
        "gd": group_done,
        "pj": group_proj,
        "mb": mix_backward,
        "mb2": mix_inner,
        "mb3": mix_outer,
        "mf": mix_finish,
    }
    for name, *rest in REDUCE_ORDER:
        reduce_steps[name](*rest)
    for copy in plain:
        copy.wait_send()
    for cond, copy in guarded:
        @pl.when(cond)
        def _():
            copy.wait_send()


def layer_stage(x, cot, small, gate, up, down, out_weight, query, key_in, value, logit):
    tok_rows, width = x.shape
    hidden_dev, features = gate.shape
    key_cols, value_cols = query.shape[1], value.shape[1]
    heads = key_cols // DK
    pieces = PIECES
    wide = features // (2 * pieces)
    vmem = pl.BlockSpec(memory_space=pltpu.VMEM)
    dma = pltpu.SemaphoreType.DMA
    f32, bf16 = jnp.float32, jnp.bfloat16
    full = (RING, tok_rows, features)
    acts = (RING, tok_rows, hidden_dev)
    block = (tok_rows, wide)
    state = (key_cols, DV)
    proj = (RING, RING, features // RING**2, value_cols)
    table = (small.shape[0], -(-max(tok_rows, key_cols) // 128) * 128)
    results = [(hidden_dev, features)] * 3 + [
        (features // RING, value_cols), query.shape, key_in.shape, value.shape, logit.shape
    ]
    return pl.pallas_call(
        layer_kernel,
        out_shape=[jax.ShapeDtypeStruct(shape, f32) for shape in results],
        in_specs=[vmem] * 11,
        out_specs=[vmem] * 8,
        scratch_shapes=[
            pltpu.VMEM((pieces, 2) + block, bf16),
            pltpu.VMEM(table, f32), pltpu.VMEM((RING,) + table, f32),
            pltpu.VMEM(state, bf16), pltpu.VMEM((RING,) + state, bf16),
            pltpu.VMEM(state, bf16), pltpu.VMEM((RING,) + state, bf16),
            pltpu.VMEM(query.shape, bf16), pltpu.VMEM(query.shape, bf16),
            pltpu.VMEM(query.shape, bf16),
            pltpu.VMEM(state, f32), pltpu.VMEM(state, bf16), pltpu.VMEM(state, f32),
            pltpu.VMEM((heads, tok_rows, tok_rows), bf16),
            pltpu.VMEM(value.shape, bf16), pltpu.VMEM(value.shape, f32),
            pltpu.VMEM(proj, bf16), pltpu.VMEM(proj, bf16),
            pltpu.VMEM(query.shape, f32), pltpu.VMEM(query.shape, f32),
            pltpu.VMEM((RING, tok_rows, 128), f32),
            pltpu.VMEM(full, bf16), pltpu.VMEM(full, bf16),
            pltpu.VMEM(acts, f32), pltpu.VMEM(acts, f32),
            pltpu.VMEM(acts, bf16), pltpu.VMEM(acts, bf16), pltpu.VMEM(acts, bf16),
            pltpu.VMEM((pieces, RING) + block, bf16), pltpu.VMEM((pieces, RING) + block, bf16),
            pltpu.VMEM((pieces, RING) + block, bf16),
            pltpu.VMEM((pieces, 2, tok_rows // 2, wide), bf16),
            pltpu.VMEM((pieces, 2) + block, bf16),
            pltpu.VMEM((pieces,) + block, bf16), pltpu.VMEM((pieces,) + block, bf16),
            pltpu.VMEM((pieces, 2) + block, bf16),
            dma((2, 3)), dma((2, 3)),
            dma((2, 2, 5)), dma((2, 2, 3)),
            dma((2, 5, 6)), dma((2, 5, 6)),
            dma((2, 4, 5)), dma((2, 4, 5)),
            dma((3,)), dma((3,)), dma((RING, 3)), dma((RING, 3)),
            dma((pieces,)), dma((pieces,)),
            dma((pieces, 2)), dma((pieces, 2)),
            dma((pieces, 4)), dma((pieces, 4)),
            dma((pieces, 2)), dma((pieces, 2)),
            dma((pieces, 2)), dma((pieces, 2)),
        ],
        compiler_params=pltpu.CompilerParams(
            collective_id=0, has_side_effects=True, vmem_limit_bytes=60 << 20
        ),
        name="layer_stage",
    )(x, cot, small, gate, up, down, out_weight, query, key_in, value, logit)


def write_kernel(*refs):
    count = len(refs) // 2
    sems = refs[-1]
    copies = [
        pltpu.make_async_copy(refs[i], refs[count + i], sems.at[i]) for i in range(count)
    ]
    for copy in copies:
        copy.start()
    for copy in copies:
        copy.wait()


def write_out(arrays):
    return pl.pallas_call(
        write_kernel,
        out_shape=[jax.ShapeDtypeStruct(a.shape, a.dtype) for a in arrays],
        in_specs=[pl.BlockSpec(memory_space=pltpu.VMEM)] * len(arrays),
        out_specs=[pl.BlockSpec(memory_space=pltpu.HBM)] * len(arrays),
        scratch_shapes=[pltpu.SemaphoreType.DMA((len(arrays),))],
        name="write_out",
    )(*arrays)


def ring_local(
    layer_in, out_cot, route_ids, route_probs, group_prob, gate_weight, up_weight,
    down_weight, out_weight, query, key_in, value, decay_logit,
):
    total = route_probs[:, 0] + route_probs[:, 1]
    expert = jnp.arange(8, dtype=jnp.int32)[:, None]
    small = sum(
        jnp.where(
            route_ids[:, j][None] == expert, (group_prob * route_probs[:, j] / total)[None], 0.0
        )
        for j in range(2)
    )
    results = write_out(layer_stage(
        layer_in, out_cot, small, gate_weight[0], up_weight[0], down_weight[0],
        out_weight, query, key_in, value, decay_logit,
    ))
    return tuple(r[None] for r in results[:3]) + tuple(results[3:])


def solution(mesh):
    in_specs = (
        P("sp", "tp"),
        P("sp", "tp"),
        P("sp", None),
        P("sp", None),
        P("sp"),
        P("sp", "tp", None),
        P("sp", "tp", None),
        P("sp", "tp", None),
        P(None, "tp"),
        P("sp", "tp"),
        P("sp", "tp"),
        P("sp", "tp"),
        P("sp", "tp"),
    )
    out_specs = (
        P("sp", "tp", None),
        P("sp", "tp", None),
        P("sp", "tp", None),
        P("sp", "tp"),
        P("sp", "tp"),
        P("sp", "tp"),
        P("sp", "tp"),
        P("sp", "tp"),
    )
    rows = 4 // mesh.shape["sp"]
    body = ring_local if rows * 4 == 4 and mesh.shape["tp"] == 8 else local
    return jax.shard_map(body, mesh=mesh, in_specs=in_specs, out_specs=out_specs, check_vma=False)
```

```python
import functools
import jax
import jax.numpy as jnp
from jax import lax
from jax.experimental import pallas as pl
from jax.experimental.pallas import tpu as pltpu
from jax.sharding import PartitionSpec as P

DK = 64
DV = 128
BLOCK = 64


decay_temp = 16.0
highest = lax.Precision.HIGH


def prefix(x, axis, join, neutral, backward):
    count = lax.axis_size(axis)
    place = lax.axis_index(axis)
    ahead = count - 1 - place if backward else place
    gathered = jax.tree.map(
        lambda a, kind: lax.all_gather(a.astype(kind), axis),
        x,
        jax.tree.map(lambda a: jnp.bfloat16 if a.dtype == jnp.float32 else a.dtype, x),
    )
    state = jax.tree.map(lambda a, e: jnp.zeros_like(a) + jnp.asarray(e, a.dtype), x, neutral)

    def one(step, state):
        source = count - 1 - step if backward else step
        return join(
            state,
            jax.tree.map(
                lambda a, own: lax.dynamic_index_in_dim(a, source, 0, False).astype(own.dtype),
                gathered,
                x,
            ),
        )

    return lax.fori_loop(0, ahead, one, state)


def combine_spans(earlier, later):
    return (earlier[0] * later[0], later[1] + later[0][..., None] * earlier[1])


def contract_rows(left_mat, right_mat):
    return lax.dot_general(
        left_mat, right_mat, (((0,), (0,)), ((), ())), preferred_element_type=jnp.float32
    )


def contract_cols(left_mat, right_mat):
    return lax.dot_general(
        left_mat, right_mat, (((1,), (1,)), ((), ())), preferred_element_type=jnp.float32
    )


def to_blocks(tensor, head_count):
    rows_here = tensor.shape[0]
    return (
        tensor.astype(jnp.float32)
        .reshape(rows_here // BLOCK, BLOCK, head_count, -1)
        .transpose(2, 0, 1, 3)
    )


def from_blocks(tensor):
    head_count, blocks, _, channels = tensor.shape
    return tensor.transpose(1, 2, 0, 3).reshape(blocks * BLOCK, head_count * channels)


def expert_pass(rows_x, rows_cot, gate_mat, up_mat, down_mat):
    full_x, full_cot = (
        lax.all_gather(rows_x, "tp", axis=1, tiled=True),
        lax.all_gather(rows_cot, "tp", axis=1, tiled=True),
    )
    gate_pre = contract_cols(full_x, gate_mat)
    up_pre = contract_cols(full_x, up_mat)
    sigmoid_gate = jax.nn.sigmoid(gate_pre)
    active = gate_pre * sigmoid_gate
    hidden = (active * up_pre).astype(jnp.bfloat16)
    hidden_cot = contract_cols(full_cot, down_mat)
    up_cot = (hidden_cot * active).astype(jnp.bfloat16)
    gate_cot = (
        hidden_cot * up_pre * sigmoid_gate * (1.0 + gate_pre * (1.0 - sigmoid_gate))
    ).astype(jnp.bfloat16)
    down_g = contract_rows(hidden, full_cot)
    gate_g = contract_rows(gate_cot, full_x)
    up_g = contract_rows(up_cot, full_x)
    dims = (((0,), (1,)), ((), ()))
    first_part = lax.dot_general(gate_mat, gate_cot, dims, preferred_element_type=jnp.float32)
    back_terms = lax.psum_scatter(
        (
            first_part + lax.dot_general(up_mat, up_cot, dims, preferred_element_type=jnp.float32)
        ).astype(jnp.bfloat16),
        "tp",
        scatter_dimension=0,
        tiled=True,
    ).astype(jnp.float32)
    return (gate_g, up_g, down_g, back_terms)


def local(
    layer_in,
    out_cot,
    route_ids,
    route_probs,
    group_prob,
    gate_weight,
    up_weight,
    down_weight,
    out_weight,
    query,
    key_in,
    value,
    decay_logit,
):
    tok_rows = layer_in.shape[0]
    local_cols = layer_in.shape[1]
    experts_all = lax.axis_size("sp")
    capacity = 4 * tok_rows // experts_all
    route_weight = group_prob[:, None] * route_probs / jnp.sum(route_probs, axis=1, keepdims=True)
    chosen = (route_ids[:, :, None] == jnp.arange(experts_all, dtype=jnp.int32)).astype(jnp.int32)
    running = jnp.cumsum(chosen.reshape(2 * tok_rows, experts_all), axis=0).reshape(
        tok_rows, 2, experts_all
    )
    position = jnp.sum((running - 1) * chosen, axis=2)
    slot_ids = route_ids * capacity + position
    matches = (
        slot_ids[None, :, :] == jnp.arange(experts_all * capacity, dtype=jnp.int32)[:, None, None]
    )
    select_x = jnp.any(matches, axis=2).astype(jnp.float32)
    select_cot = jnp.sum(jnp.where(matches, route_weight[None], 0.0), axis=2)
    send_x = jnp.dot(
        select_x.astype(jnp.bfloat16), layer_in, preferred_element_type=jnp.float32
    ).astype(jnp.bfloat16)
    send_cot = jnp.dot(select_cot, out_cot.astype(jnp.float32), precision=highest).astype(
        jnp.bfloat16
    )
    send_x = send_x.reshape(experts_all, capacity, local_cols)
    send_cot = send_cot.reshape(experts_all, capacity, local_cols)
    recv_x, recv_cot = (
        lax.all_to_all(send_x, "sp", split_axis=0, concat_axis=0, tiled=True),
        lax.all_to_all(send_cot, "sp", split_axis=0, concat_axis=0, tiled=True),
    )
    head_dev = query.shape[1] // DK
    scaled_query = to_blocks(query, head_dev) * DK ** (-0.5)
    key_blk = to_blocks(key_in, head_dev)
    value_blk = to_blocks(value, head_dev)
    logit_blk = to_blocks(decay_logit, head_dev)
    cumulative = jnp.cumsum(jax.nn.log_sigmoid(logit_blk) / decay_temp, axis=2)
    span_log = cumulative[:, :, -1:, :]
    growth = jnp.exp(cumulative)
    shrink = jnp.exp(-cumulative)
    to_end = jnp.exp(span_log - cumulative)
    query_decayed = scaled_query * growth
    key_back = key_blk * shrink
    key_to_end = key_blk * to_end
    causal = jnp.tril(jnp.ones((BLOCK, BLOCK), dtype=bool))
    scores = jnp.where(
        causal, jnp.einsum("hncd,hnsd->hncs", query_decayed, key_back, precision=highest), 0.0
    )
    within = jnp.einsum("hncs,hnsv->hncv", scores, value_blk, precision=highest)
    block_decay = jnp.moveaxis(jnp.exp(span_log[:, :, 0, :]), 1, 0)
    block_update = jnp.moveaxis(
        jnp.einsum("hncd,hncv->hndv", key_to_end, value_blk, precision=highest), 1, 0
    )
    identity_pair = (
        jnp.ones((head_dev, DK), jnp.float32),
        jnp.zeros((head_dev, DK, DV), jnp.float32),
    )

    def advance(carry_pair, inputs):
        return (combine_spans(carry_pair, inputs), carry_pair)

    span_total, before_pairs = lax.scan(advance, identity_pair, (block_decay, block_update))
    entry_pair = prefix(span_total, "sp", combine_spans, identity_pair, False)
    entry_state = entry_pair[1]
    decay_before = jnp.moveaxis(before_pairs[0], 0, 1)
    block_state = decay_before[..., None] * entry_state[:, None] + jnp.moveaxis(
        before_pairs[1], 0, 1
    )
    span_end = span_total[0][..., None] * entry_state + span_total[1]
    outputs = within + jnp.einsum("hncd,hndv->hncv", query_decayed, block_state, precision=highest)
    mixer_out = from_blocks(outputs).astype(jnp.bfloat16)
    gate_mat, up_mat, down_mat = (gate_weight[0], up_weight[0], down_weight[0])
    gate_g, up_g, down_g, back_flat = expert_pass(
        recv_x.reshape(-1, local_cols), recv_cot.reshape(-1, local_cols), gate_mat, up_mat, down_mat
    )
    back_terms = back_flat.reshape(local_cols, experts_all, capacity)
    returned = lax.all_to_all(
        back_terms.astype(jnp.bfloat16), "sp", split_axis=1, concat_axis=1, tiled=True
    ).astype(back_terms.dtype)
    returned = returned.reshape(local_cols, experts_all * capacity)
    routed_sum = lax.dot_general(
        select_x,
        returned,
        (((0,), (1,)), ((), ())),
        precision=highest,
        preferred_element_type=jnp.float32,
    )
    mixed_cot = (out_cot.astype(jnp.float32) + routed_sum).astype(jnp.bfloat16)
    full_cot = lax.all_gather(mixed_cot, "tp", axis=1, tiled=True)
    mixer_cot = jnp.dot(full_cot, out_weight, preferred_element_type=jnp.float32)
    proj_grad = lax.psum_scatter(
        contract_rows(full_cot, mixer_out).astype(jnp.bfloat16),
        "sp",
        scatter_dimension=0,
        tiled=True,
    ).astype(jnp.float32)
    cot_blk = to_blocks(mixer_cot, head_dev)
    block_future = jnp.moveaxis(
        jnp.einsum("hncd,hncv->hndv", query_decayed, cot_blk, precision=highest), 1, 0
    )

    def retreat(carry_pair, inputs):
        return (combine_spans(carry_pair, inputs), carry_pair)

    span_back, after_pairs = lax.scan(
        retreat, identity_pair, (block_decay, block_future), reverse=True
    )
    beyond_pair = prefix(span_back, "sp", combine_spans, identity_pair, True)
    future_state = beyond_pair[1]
    decay_after = jnp.moveaxis(after_pairs[0], 0, 1)
    block_future_state = decay_after[..., None] * future_state[:, None] + jnp.moveaxis(
        after_pairs[1], 0, 1
    )
    cot_values = jnp.where(
        causal, jnp.einsum("hncv,hnsv->hncs", cot_blk, value_blk, precision=highest), 0.0
    )
    query_scaled_grad = growth * (
        jnp.einsum("hncv,hndv->hncd", cot_blk, block_state, precision=highest)
        + jnp.einsum("hncs,hnsd->hncd", cot_values, key_back, precision=highest)
    )
    key_part = shrink * jnp.einsum("hncs,hncd->hnsd", cot_values, query_decayed, precision=highest)
    key_grad = key_part + to_end * jnp.einsum(
        "hnsv,hndv->hnsd", value_blk, block_future_state, precision=highest
    )
    value_grad = jnp.einsum("hncs,hncv->hnsv", scores, cot_blk, precision=highest) + jnp.einsum(
        "hnsd,hndv->hnsv", key_to_end, block_future_state, precision=highest
    )
    decay_terms = (scaled_query * query_scaled_grad - key_blk * key_grad).reshape(
        head_dev, tok_rows, DK
    )
    tail_sum = jnp.flip(jnp.cumsum(jnp.flip(decay_terms, 1), axis=1), 1)
    beyond_term = jnp.sum(future_state * span_end, axis=2)
    log_grad = tail_sum + beyond_term[:, None, :]
    logit_flat = logit_blk.reshape(head_dev, tok_rows, DK)
    logit_grad = (
        (log_grad * jax.nn.sigmoid(-logit_flat) / decay_temp)
        .transpose(1, 0, 2)
        .reshape(tok_rows, head_dev * DK)
    )
    query_grad = from_blocks(query_scaled_grad * DK ** (-0.5))
    return (
        gate_g[None],
        up_g[None],
        down_g[None],
        proj_grad,
        query_grad,
        from_blocks(key_grad),
        from_blocks(value_grad),
        logit_grad,
    )


RING = 4
EXPERT_CUT = 5
PIECES = 8
GATHER_ORDER = (
    ("zs", 0, 0),
    ("rs", 1, 4),
    ("rs", 0, 4),
    ("zs", 1, 0),
    ("rs", 0, 0),
    ("rf", 0, 4, 1),
    ("rf", 1, 4, 1),
    ("prep",),
    ("rf", 1, 4, 0),
    ("rf", 0, 4, 0),
    ("rn", 0, 4),
    ("zr", 0, 0, 1),
    ("rf", 0, 0, 1),
    ("rs", 1, 0),
    ("rn", 1, 4),
    ("zr", 0, 0, 2),
    ("zr", 1, 0, 1),
    ("ro", 1, 4),
    ("ro", 0, 4),
    ("rf", 0, 1, 0),
    ("zr", 0, 0, 3),
    ("rf", 0, 1, 1),
    ("zr", 1, 1, 1),
    ("zr", 1, 0, 2),
    ("rf", 1, 0, 1),
    ("zr", 0, 1, 2),
    ("rn", 0, 1),
    ("rf", 1, 1, 0),
    ("rf", 0, 0, 0),
    ("rf", 0, 2, 0),
    ("mixf",),
    ("rf", 1, 1, 1),
    ("rf", 0, 2, 1),
    ("rn", 0, 0),
    ("rn", 1, 1),
    ("zr", 1, 1, 3),
    ("fx", 0),
    ("zr", 0, 1, 1),
    ("rf", 1, 0, 0),
    ("rn", 1, 0),
    ("rf", 0, 3, 1),
    ("rf", 0, 3, 0),
    ("rn", 0, 2),
    ("rn", 0, 3),
    ("zr", 1, 0, 3),
    ("fx", 1),
    ("rf", 1, 2, 1),
    ("rf", 1, 2, 0),
    ("zr", 0, 1, 3),
    ("fx", 3),
    ("ro", 0, 1),
    ("rn", 1, 2),
    ("sy", 0),
    ("zr", 1, 1, 2),
    ("rf", 1, 3, 0),
    ("ro", 0, 3),
    ("rf", 1, 3, 1),
    ("rn", 1, 3),
    ("ro", 0, 0),
    ("ro", 1, 1),
    ("fx", 4),
    ("sy", 4),
    ("ro", 0, 2),
    ("ro", 1, 0),
    ("ro", 1, 2),
    ("sy", 3),
    ("ro", 1, 3),
    ("sy", 1),
    ("fx", 2),
    ("sy", 2),
)
REDUCE_ORDER = (
    ("pt", 0),
    ("pt", 1),
    ("op", 0),
    ("pt", 2),
    ("g", 1),
    ("op", 1),
    ("pt", 3),
    ("rl", 0, 0),
    ("rl", 2, 0),
    ("rl", 0, 1),
    ("op", 2),
    ("to", 2, 0),
    ("rl", 1, 1),
    ("to", 0, 0),
    ("rl", 3, 1),
    ("g", 8),
    ("rl", 2, 1),
    ("rl", 3, 0),
    ("rl", 4, 0),
    ("rl", 4, 1),
    ("rl", 1, 0),
    ("to", 0, 1),
    ("g", 7),
    ("g", 11),
    ("g", 3),
    ("rl", 5, 1),
    ("rl", 5, 0),
    ("mi", 2, 0),
    ("op", 3),
    ("mi", 0, 0),
    ("mi", 0, 1),
    ("to", 1, 1),
    ("to", 3, 1),
    ("to", 3, 0),
    ("g", 6),
    ("to", 1, 0),
    ("mi", 1, 1),
    ("to", 2, 1),
    ("to", 4, 1),
    ("to", 5, 0),
    ("g", 4),
    ("mi", 3, 1),
    ("to", 4, 0),
    ("rl", 6, 1),
    ("rl", 6, 0),
    ("g", 9),
    ("g", 5),
    ("lt", 0, 0),
    ("mi", 3, 0),
    ("rl", 7, 0),
    ("to", 5, 1),
    ("rl", 7, 1),
    ("mi", 1, 0),
    ("lt", 1, 1),
    ("to", 6, 1),
    ("lt", 0, 1),
    ("to", 6, 0),
    ("mi", 2, 1),
    ("mi", 4, 1),
    ("lt", 3, 1),
    ("mi", 4, 0),
    ("to", 7, 0),
    ("to", 7, 1),
    ("mi", 5, 0),
    ("gd", 0),
    ("lt", 1, 0),
    ("lt", 3, 0),
    ("lt", 2, 0),
    ("gd", 1),
    ("pj", 0),
    ("mi", 5, 1),
    ("lt", 4, 1),
    ("lt", 2, 1),
    ("mi", 6, 1),
    ("lt", 4, 0),
    ("gd", 2),
    ("gd", 3),
    ("mi", 6, 0),
    ("lt", 5, 0),
    ("pj", 1),
    ("mi", 7, 0),
    ("g", 10),
    ("lt", 5, 1),
    ("mi", 7, 1),
    ("gd", 4),
    ("g", 0),
    ("lt", 6, 1),
    ("gd", 5),
    ("pj", 2),
    ("lt", 6, 0),
    ("lt", 7, 0),
    ("lt", 7, 1),
    ("gd", 6),
    ("gd", 7),
    ("mb",),
    ("mb2",),
    ("pj", 3),
    ("g", 2),
    ("mb3",),
    ("mf",),
)


def ring_place(index):
    return index + (index // 2) * (1 - 2 * (index % 2))


def remote(source, target, send_sem, recv_sem, device):
    return pltpu.make_async_remote_copy(
        src_ref=source,
        dst_ref=target,
        send_sem=send_sem,
        recv_sem=recv_sem,
        device_id=device,
        device_id_type=pl.DeviceIdType.MESH,
    )


def greet(devices):
    barrier = pltpu.get_barrier_semaphore()
    for device in devices:
        pl.semaphore_signal(
            barrier, inc=1, device_id=device, device_id_type=pl.DeviceIdType.MESH
        )
    pl.semaphore_wait(barrier, len(devices))


def arrived(sem, region):
    pltpu.make_async_copy(region, region, sem).wait()


class Place:
    def __init__(self):
        self.sp, self.tp = lax.axis_index("sp"), lax.axis_index("tp")
        self.z, self.core = self.tp // 2, self.tp % 2
        ring = ring_place(self.sp)
        self.at = [ring_place((ring + step) % RING) for step in range(RING)]
        self.right, self.across, self.left = [(self.at[s], self.tp) for s in (1, 2, 3)]
        self.pair = (self.sp, 2 * self.z + 1 - self.core)
        self.near = (self.sp, 2 * (self.z + 1 - 2 * (self.z % 2)) + self.core)
        self.far = (self.sp, 2 * (RING - 1 - self.z) + self.core)
        upper = self.z // 2
        folded = self.z + upper * (RING - 1 - 2 * self.z)
        self.inner = folded == 1
        self.end = folded == 0
        order = [folded, 1 - folded, 2, 3]
        self.slot = [o + upper * (RING - 1 - 2 * o) for o in order]


def layer_kernel(
    x_far, cot_far, ids_far, probs_far, group_far, gate_far, up_far, down_far, out_far,
    query_far, key_far, value_far, logit_far,
    gate_out, up_out, down_out, proj_out, query_out, key_out, value_out, logit_out,
    x_ref, cot_ref, ids_ref, probs_ref, group_ref, gate_ref, up_ref, down_ref, out_ref,
    query_ref, key_ref, value_ref, logit_ref, load_sem,
    mixed, small_buf, small_out, state_buf, state_out, future_buf, future_out,
    decayed, key_back, key_end, state_own, entry, span_end, scores, mixer_out, mixer_cot,
    proj_to, proj_from, summed, terms, weights,
    x_all, cot_all, gate_pre, up_pre, hidden, gate_cot, up_cot,
    pair_to, pair_from, parts, first_in, second_in, total, half_total, z_in,
    tiny_send, tiny_recv, zs, zr, ps, pr, qs, qr,
    fs, fr, js, jr, bs, br, r1s, r1r, r2s, r2r, zts, ztr, ms, mr,
):
    here = Place()
    loads = [
        pltpu.make_async_copy(far, near, load_sem.at[i])
        for i, (far, near) in enumerate((
            (x_far, x_ref), (cot_far, cot_ref), (ids_far, ids_ref), (probs_far, probs_ref),
            (group_far, group_ref), (query_far, query_ref), (key_far, key_ref),
            (value_far, value_ref), (logit_far, logit_ref), (gate_far, gate_ref),
            (up_far, up_ref), (down_far, down_ref), (out_far, out_ref),
        ))
    ]
    for copy in loads:
        copy.start()
    tok_rows, width = x_ref.shape
    lead = tok_rows * 4 // EXPERT_CUT
    tail = tok_rows - lead
    ins, alls = (x_ref, cot_ref), (x_all, cot_all)
    greet([here.right, here.across, here.left, here.near, here.far, here.pair])
    for copy in loads[:2]:
        copy.wait()
    plain, guarded = [], []

    def go(source, target, send_sem, recv_sem, device):
        copy = remote(source, target, send_sem, recv_sem, device)
        copy.start()
        plain.append(copy)

    def go_if(cond, source, target, send_sem, recv_sem, device):
        copy = remote(source, target, send_sem, recv_sem, device)

        @pl.when(cond)
        def _():
            copy.start()

        guarded.append((cond, copy))

    def cols(slot, core):
        return pl.ds(pl.multiple_of((2 * here.slot[slot] + core) * width, width), width)

    def piece(a, part, slot, core=None):
        core = here.core if core is None else core
        if part == 0:
            return alls[a].at[here.sp, pl.ds(0, lead), cols(slot, core)]
        return alls[a].at[:, pl.ds(lead, tail), cols(slot, core)]

    def own_rows(a, start, count):
        return ins[a].at[pl.ds(start, count), :]

    def z_start(a, part):
        source = own_rows(a, 0, lead) if part == 0 else piece(a, 1, 0)
        target = piece(a, part, 0)
        go(source, target, zs.at[a, part, 0], zr.at[a, part, 0], here.near)
        go_if(here.inner, source, target, zs.at[a, part, 1], zr.at[a, part, 1], here.far)

    def z_relay(a, part, slot):
        region = piece(a, part, slot)
        arrived(zr.at[a, part, slot - 1], region)
        if slot == 1:
            go_if(here.inner, region, region, zs.at[a, part, 2], zr.at[a, part, 2], here.far)
        else:
            go_if(
                here.inner, region, region, zs.at[a, part, slot + 1], zr.at[a, part, slot - 1],
                here.near,
            )
        if part == 0:
            pair_send(a, slot, 0)
            ring_send(a, (slot, 0))
        else:
            go(region, region, qs.at[a, slot, 4], qr.at[a, slot, 4], here.pair)

    def bounds(part, h):
        start, count = (0, lead) if part == 0 else (lead, tail)
        return start + h * (count // 2), count // 2

    def ring_region(a, unit, step, h):
        slot, part = unit
        start, count = bounds(part, h)
        return alls[a].at[here.at[step], pl.ds(start, count), cols(slot, here.core)]

    def number(unit):
        return unit[0] + 4 * unit[1]

    def ring_send(a, unit):
        slot, part = unit
        n = number(unit)
        for i, (h, device) in enumerate(
            ((0, here.right), (1, here.right), (0, here.left), (1, here.left))
        ):
            start, count = bounds(part, h)
            source = own_rows(a, start, count) if slot == 0 else ring_region(a, unit, 0, h)
            copy = remote(source, ring_region(a, unit, 0, h), ps.at[a, n, i], pr.at[a, n, i], device)
            plain.append(copy)
        right0, right1, left0, left1 = plain[-4:]
        for copy in (right0, left1, right1, left0):
            copy.start()

    def ring_forward(a, unit, h):
        n = number(unit)
        region = ring_region(a, unit, (3, 1)[h], h)
        arrived(pr.at[a, n, 3 * h], region)
        go(region, region, ps.at[a, n, 4 + h], pr.at[a, n, 4 + h], (here.right, here.left)[h])

    def ring_near(a, unit):
        n = number(unit)
        arrived(pr.at[a, n, 1], ring_region(a, unit, 3, 1))
        arrived(pr.at[a, n, 2], ring_region(a, unit, 1, 0))
        if unit[1] == 0:
            pair_send(a, unit[0], 1)
            pair_send(a, unit[0], 3)

    def ring_across(a, unit):
        n = number(unit)
        arrived(pr.at[a, n, 4], ring_region(a, unit, 2, 0))
        arrived(pr.at[a, n, 5], ring_region(a, unit, 2, 1))
        if unit[1] == 0:
            pair_send(a, unit[0], 2)
        else:
            z_start(a, 1)
            region = piece(a, 1, 0)
            go(region, region, qs.at[a, 0, 4], qr.at[a, 0, 4], here.pair)

    def pair_region(a, slot, step, core):
        return alls[a].at[here.at[step], pl.ds(0, lead), cols(slot, core)]

    def pair_send(a, slot, step):
        region = pair_region(a, slot, step, here.core)
        source = own_rows(a, 0, lead) if slot == 0 and step == 0 else region
        go(source, region, qs.at[a, slot, step], qr.at[a, slot, step], here.pair)

    def pair_wait(a, step):
        for slot in range(RING):
            if step < 4:
                arrived(qr.at[a, slot, step], pair_region(a, slot, step, 1 - here.core))
            else:
                arrived(qr.at[a, slot, 4], piece(a, 1, slot, 1 - here.core))

    bf16, f32 = jnp.bfloat16, jnp.float32
    key_cols = query_ref.shape[1]
    heads = key_cols // DK
    lane = lax.broadcasted_iota(jnp.int32, (1, key_cols), 1) // DK
    row = lax.broadcasted_iota(jnp.int32, (key_cols, 1), 0) // DK

    def dot(left, right, left_dim=1, right_dim=0, precision=None):
        return lax.dot_general(
            left, right, (((left_dim,), (right_dim,)), ((), ())),
            precision=precision, preferred_element_type=f32,
        )

    def two(value):
        high = value.astype(bf16)
        return high, (value - high.astype(f32)).astype(bf16)

    def triangle():
        return lax.broadcasted_iota(jnp.int32, (tok_rows, tok_rows), 0) >= (
            lax.broadcasted_iota(jnp.int32, (tok_rows, tok_rows), 1)
        )

    def only(value, h):
        return jnp.where(lane == h, value, jnp.zeros_like(value))

    def join(parts_of, which):
        joined = parts_of[0]
        for h in range(1, heads):
            joined = jnp.where(which == h, parts_of[h], joined)
        return joined

    def head_cols(h):
        return pl.ds(h * DV, DV)

    def log_decay(logit):
        return -(jnp.maximum(-logit, 0.0) + jnp.log(1.0 + jnp.exp(-jnp.abs(logit)))) / decay_temp

    def column(s):
        pick = (
            lax.broadcasted_iota(jnp.int32, (small_buf.shape[0], DV), 0) == RING
        ).astype(f32)
        return dot(
            small_out[s, :, pl.ds(0, key_cols)], pick, 0, 0, lax.Precision.HIGHEST
        )

    def mix_prepare():
        for copy in loads[2:]:
            copy.wait()
        ones = triangle().astype(bf16)
        high, low = two(log_decay(logit_ref[...].astype(f32)))
        cumulative = dot(ones, high) + dot(ones, low)
        summed[...] = cumulative
        last = cumulative[tok_rows - 1 : tok_rows, :]
        keys = key_ref[...].astype(f32)
        decayed[...] = (
            query_ref[...].astype(f32) * DK ** (-0.5) * jnp.exp(cumulative)
        ).astype(bf16)
        key_back[...] = (keys * jnp.exp(-cumulative)).astype(bf16)
        ends = (keys * jnp.exp(last - cumulative)).astype(bf16)
        key_end[...] = ends
        state = join([dot(ends, value_ref[:, head_cols(h)], 0, 0) for h in range(heads)], row)
        state_own[...] = state
        state_buf[...] = state.astype(bf16)
        share = group_ref[...].reshape(1, tok_rows) / (probs_ref[0:1, :] + probs_ref[1:2, :])
        expert = lax.broadcasted_iota(jnp.int32, (small_buf.shape[0], tok_rows), 0)
        small_buf[...] = jnp.zeros_like(small_buf)
        small_buf[:, pl.ds(0, tok_rows)] = sum(
            jnp.where(ids_ref[j : j + 1, :] == expert, share * probs_ref[j : j + 1, :], 0.0)
            for j in range(2)
        )
        small_buf[RING : RING + 1, pl.ds(0, key_cols)] = jnp.exp(last)
        small_out[here.sp] = small_buf[...]
        state_out[here.sp] = state_buf[...]
        for i, (buf, out) in enumerate(((small_buf, small_out), (state_buf, state_out))):
            for step, device in ((1, here.right), (3, here.left), (2, here.across)):
                go(
                    buf, out.at[here.sp], tiny_send.at[i, step - 1], tiny_recv.at[i, 3 - step],
                    device,
                )

    def mix_forward():
        for step in (1, 2, 3):
            arrived(tiny_recv.at[0, step - 1], small_out.at[here.at[step]])
            arrived(tiny_recv.at[1, step - 1], state_out.at[here.at[step]])
        state = jnp.zeros((key_cols, DV), f32)
        for s in range(RING - 1):
            later = state * column(s) + state_out[s].astype(f32)
            state = jnp.where(here.sp > s, later, state)
        entry[...] = state.astype(bf16)
        mine = (
            lax.broadcasted_iota(jnp.int32, (small_buf.shape[0], 128), 0) == here.sp
        ).astype(f32)
        for s in range(RING):
            weights[s] = dot(small_out[s], mine, 0, 0, lax.Precision.HIGHEST)[:tok_rows]
        span_end[...] = state * column(here.sp) + state_own[...]
        keep = triangle()
        for h in range(heads):
            mine = only(decayed[...], h)
            score = jnp.where(keep, dot(mine, key_back[...], 1, 1), 0.0).astype(bf16)
            scores[h] = score
            mixer_out[:, head_cols(h)] = (
                dot(score, value_ref[:, head_cols(h)]) + dot(mine, entry[...])
            ).astype(bf16)

    def mix_backward():
        cot = [mixer_cot[:, head_cols(h)].astype(bf16) for h in range(heads)]
        future = join([dot(decayed[...], cot[h], 0, 0) for h in range(heads)], row)
        future_buf[...] = future.astype(bf16)
        for step, device in ((1, here.right), (3, here.left), (2, here.across)):
            go(
                future_buf, future_out.at[here.sp], fs.at[step - 1], fr.at[3 - step], device
            )

    held = {}

    def mix_inner():
        keep = triangle()
        cot = [mixer_cot[:, head_cols(h)].astype(bf16) for h in range(heads)]
        pairs = [
            jnp.where(keep, dot(cot[h], value_ref[:, head_cols(h)], 1, 1), 0.0).astype(bf16)
            for h in range(heads)
        ]
        inner = join(
            [dot(cot[h], entry[...], 1, 1) + dot(pairs[h], key_back[...]) for h in range(heads)],
            lane,
        )
        key_inner = join([dot(pairs[h], decayed[...], 0, 0) for h in range(heads)], lane)
        query_out[...] = jnp.exp(summed[...]) * inner * DK ** (-0.5)
        key_out[...] = jnp.exp(-summed[...]) * key_inner
        terms[...] = (
            decayed[...].astype(f32) * inner - key_back[...].astype(f32) * key_inner
        )
        for h in range(heads):
            value_out[:, head_cols(h)] = dot(scores[h], cot[h], 0, 0)

    def mix_outer():
        for step in (1, 2, 3):
            arrived(fr.at[step - 1], future_out.at[here.at[step]])
        state = jnp.zeros((key_cols, DV), f32)
        for s in range(RING - 1, 0, -1):
            earlier = state * column(s) + future_out[s].astype(f32)
            state = jnp.where(here.sp < s, earlier, state)
        ahead = state.astype(bf16)
        key_outer = join(
            [dot(value_ref[:, head_cols(h)], ahead, 1, 1) for h in range(heads)], lane
        )
        last = summed[tok_rows - 1 : tok_rows, :]
        key_out[...] += jnp.exp(last - summed[...]) * key_outer
        for h in range(heads):
            value_out[:, head_cols(h)] += dot(only(key_end[...], h), ahead)
        high, low = two(terms[...] - key_end[...].astype(f32) * key_outer)
        ones = triangle().astype(bf16)
        tail_sum = dot(ones, high, 0, 0) + dot(ones, low, 0, 0)
        beyond = dot(
            jnp.ones((8, DV), f32), state * span_end[...], 1, 1, lax.Precision.HIGHEST
        )[0:1, :]
        logit_out[...] = (tail_sum + beyond) / (
            decay_temp * (1.0 + jnp.exp(logit_ref[...].astype(f32)))
        )

    def mix_finish():
        for m in range(RING):
            result = proj_to[m, here.sp].astype(f32)
            for step in (1, 3, 2):
                arrived(jr.at[m, step - 1], proj_from.at[m, here.at[step]])
                result = result + proj_from[m, here.at[step]].astype(f32)
            proj_out[pl.ds(m * atom, atom), :] = result

    def block_of(ref, s):
        if s is None:
            return ref[:, pl.ds(lead, tail), :].reshape(RING * tail, ref.shape[2])
        return ref[s, pl.ds(0, lead), :]

    def keep_block(ref, s, value):
        if s is None:
            ref[:, pl.ds(lead, tail), :] = value.reshape(RING, tail, ref.shape[2])
        else:
            ref[s, pl.ds(0, lead), :] = value

    def forward_rows(s):
        block = block_of(x_all, s)
        keep_block(gate_pre, s, contract_cols(block, gate_ref[...]))
        keep_block(up_pre, s, contract_cols(block, up_ref[...]))

    def second_rows(s):
        weight = jnp.concatenate([block_of(weights, s)] * (width // 128), axis=1)
        hidden_cot = contract_cols(block_of(cot_all, s), down_ref[...]) * weight
        gp, upp = block_of(gate_pre, s), block_of(up_pre, s)
        sig = 1.0 / (1.0 + jnp.exp(-gp))
        active = gp * sig
        keep_block(hidden, s, (active * upp * weight).astype(jnp.bfloat16))
        keep_block(up_cot, s, (hidden_cot * active).astype(jnp.bfloat16))
        keep_block(
            gate_cot, s,
            (hidden_cot * upp * sig * (1.0 + gp * (1.0 - sig))).astype(jnp.bfloat16),
        )

    def rows_of(a, step, work):
        pair_wait(a, step)
        work(here.at[step] if step < RING else None)

    def own_start(a):
        ring_send(a, (0, 0))
        pair_send(a, 0, 0)

    gather_steps = {
        "zs": z_start,
        "rs": lambda a, n: own_start(a) if n == 0 else ring_send(a, (0, 1)),
        "zr": z_relay,
        "rf": lambda a, n, h: ring_forward(a, (n % 4, n // 4), h),
        "rn": lambda a, n: ring_near(a, (n % 4, n // 4)),
        "ro": lambda a, n: ring_across(a, (n % 4, n // 4)),
        "prep": mix_prepare,
        "mixf": mix_forward,
        "fx": lambda i: rows_of(0, i, forward_rows),
        "sy": lambda i: rows_of(1, i, second_rows),
    }
    for a in range(2):
        alls[a][here.sp, :, cols(0, here.core)] = ins[a][...]
    for name, *rest in GATHER_ORDER:
        gather_steps[name](*rest)

    pieces, wide = parts.shape[0], parts.shape[3]
    split = tok_rows // 2
    span = gate_ref.shape[1] // RING
    atom = span // RING
    per = 2 * atom // wide

    def atoms(k, core):
        for i in range(wide // atom):
            target = 2 * core + (k % per) + i
            yield pl.ds(pl.multiple_of(target * span + (k // per) * atom, atom), atom)

    def columns(ref, k, core):
        return jnp.concatenate([ref[:, c] for c in atoms(k, core)], axis=1)

    top, bottom = pl.ds(0, split), pl.ds(split, split)

    def partial(m, core):
        rows = RING * tok_rows
        total_of = [
            jnp.dot(
                cot[...].reshape(rows, width),
                jnp.concatenate([columns(ref, m * per + i, core) for i in range(per)], axis=1),
                preferred_element_type=jnp.float32,
            )
            for cot, ref in ((gate_cot, gate_ref), (up_cot, up_ref))
        ]
        both = total_of[0] + total_of[1]
        for i in range(per):
            part = both[:, i * wide : (i + 1) * wide]
            yield m * per + i, part.reshape(RING, tok_rows, wide)

    def pair_part(m):
        for k, part in partial(m, 1 - here.core):
            pair_to[k] = part.astype(jnp.bfloat16)
            go(pair_to.at[k], pair_from.at[k], bs.at[k], br.at[k], here.pair)

    def own_part(m):
        for k, part in partial(m, here.core):
            arrived(br.at[k], pair_from.at[k])
            parts[k] = (part + pair_from[k].astype(jnp.float32)).astype(jnp.bfloat16)
            right, across, left = [parts.at[k, here.at[i]] for i in (1, 2, 3)]
            go(across.at[top], first_in.at[k, 0], r1s.at[k, 0], r1r.at[k, 0], here.right)
            go(across.at[bottom], first_in.at[k, 1], r1s.at[k, 1], r1r.at[k, 1], here.left)
            go(
                right.at[bottom], second_in.at[k, 0, bottom], r2s.at[k, 0], r2r.at[k, 0],
                here.right,
            )
            go(left.at[top], second_in.at[k, 1, top], r2s.at[k, 1], r2r.at[k, 1], here.left)

    def add_to(ref, other):
        ref[...] = (ref[...].astype(jnp.float32) + other.astype(jnp.float32)).astype(jnp.bfloat16)

    def ring_relay(k, h):
        step, rows, device = ((1, top, here.right), (3, bottom, here.left))[h]
        arrived(r1r.at[k, h], first_in.at[k, h])
        mine = parts.at[k, here.at[step]].at[rows]
        add_to(mine, first_in[k, h])
        go(
            mine, second_in.at[k, h, rows],
            r2s.at[k, 2 + h], r2r.at[k, 2 + h], device,
        )

    halves = (top, bottom)

    def ring_total(k, h):
        rows = halves[h]
        own_sem, sum_sem = ((1, 2), (0, 3))[h]
        own_from, sum_from = ((1, 0), (0, 1))[h]
        arrived(r2r.at[k, own_sem], second_in.at[k, own_from, rows])
        arrived(r2r.at[k, sum_sem], second_in.at[k, sum_from, rows])
        total[k, rows] = (
            parts[k, here.sp, rows].astype(jnp.float32)
            + second_in[k, 0, rows].astype(jnp.float32)
            + second_in[k, 1, rows].astype(jnp.float32)
        ).astype(jnp.bfloat16)
        go_if(
            here.end, total.at[k, rows], z_in.at[k, 0, rows], zts.at[k, h, 0], ztr.at[k, h, 0],
            here.near,
        )

    def line_middle(k, h):
        rows = halves[h]
        copy = remote(
            half_total.at[k, rows], z_in.at[k, 1, rows], zts.at[k, h, 1], ztr.at[k, h, 1], here.far
        )

        @pl.when(here.inner)
        def _():
            arrived(ztr.at[k, h, 0], z_in.at[k, 0, rows])
            half_total[k, rows] = (
                total[k, rows].astype(jnp.float32) + z_in[k, 0, rows].astype(jnp.float32)
            ).astype(jnp.bfloat16)
            copy.start()

        guarded.append((here.inner, copy))

    def line_total(k, h):
        rows = halves[h]
        region = mixed.at[k, here.core, rows]
        copy = remote(region, region, ms.at[k, h, 0], mr.at[k, h, 0], here.near)

        @pl.when(here.inner)
        def _():
            arrived(ztr.at[k, h, 1], z_in.at[k, 1, rows])
            mixed[k, here.core, rows] = (
                columns(cot_all.at[here.sp, rows], k, here.core).astype(jnp.float32)
                + (
                    half_total[k, rows].astype(jnp.float32)
                    + z_in[k, 1, rows].astype(jnp.float32)
                )
            ).astype(jnp.bfloat16)
            copy.start()

        guarded.append((here.inner, copy))

        @pl.when(here.end)
        def _():
            arrived(mr.at[k, h, 0], region)

        go(region, region, ms.at[k, h, 1], mr.at[k, h, 1], here.pair)

    features = gate_ref.shape[1]
    block_cols = 2 * width

    def weight_grad(n):
        which, j = n % 3, n // 3
        left, right, out = (
            (gate_cot, x_all, gate_out), (up_cot, x_all, up_out), (hidden, cot_all, down_out)
        )[which]
        c = pl.ds(j * block_cols, block_cols)
        rows = RING * tok_rows
        out[:, c] = contract_rows(
            left[...].reshape(rows, width), right[:, :, c].reshape(rows, block_cols)
        )

    def mixed_group(m):
        return jnp.concatenate(
            [mixed[m * per + i, core] for core in range(2) for i in range(per)], axis=1
        )

    def group_done(k):
        for h in range(2):
            arrived(mr.at[k, h, 1], mixed.at[k, 1 - here.core, halves[h]])
        if (k + 1) % per:
            return
        m = k // per
        group = mixed_group(m)
        weight = jnp.concatenate(
            [out_ref[pl.ds(d * span + m * atom, atom), :] for d in range(RING)], axis=0
        )
        term = dot(group, weight)
        mixer_cot[...] = term if m == 0 else mixer_cot[...] + term

    def group_proj(m):
        group = mixed_group(m)
        block = dot(group, mixer_out[...], 0, 0).astype(bf16)
        for d in range(RING):
            proj_to[m, d] = block[d * atom : (d + 1) * atom, :]
        for step, device in ((1, here.right), (3, here.left), (2, here.across)):
            go(
                proj_to.at[m, here.at[step]], proj_from.at[m, here.sp],
                js.at[m, step - 1], jr.at[m, 3 - step], device,
            )

    reduce_steps = {
        "pt": pair_part,
        "op": own_part,
        "g": weight_grad,
        "rl": ring_relay,
        "to": ring_total,
        "mi": line_middle,
        "lt": line_total,
        "gd": group_done,
        "pj": group_proj,
        "mb": mix_backward,
        "mb2": mix_inner,
        "mb3": mix_outer,
        "mf": mix_finish,
    }
    for name, *rest in REDUCE_ORDER:
        reduce_steps[name](*rest)
    for copy in plain:
        copy.wait_send()
    for cond, copy in guarded:
        @pl.when(cond)
        def _():
            copy.wait_send()


def layer_stage(*inputs):
    x, _, _, _, _, gate, _, _, _, query, key_in, value, logit = inputs
    tok_rows, width = x.shape
    hidden_dev, features = gate.shape
    key_cols, value_cols = query.shape[1], value.shape[1]
    heads = key_cols // DK
    pieces = PIECES
    wide = features // (2 * pieces)
    vmem = pl.BlockSpec(memory_space=pltpu.VMEM)
    dma = pltpu.SemaphoreType.DMA
    f32, bf16 = jnp.float32, jnp.bfloat16
    full = (RING, tok_rows, features)
    acts = (RING, tok_rows, hidden_dev)
    block = (tok_rows, wide)
    state = (key_cols, DV)
    proj = (RING, RING, features // RING**2, value_cols)
    table = (8, -(-max(tok_rows, key_cols) // 128) * 128)
    results = [(hidden_dev, features)] * 3 + [
        (features // RING, value_cols), query.shape, key_in.shape, value.shape, logit.shape
    ]
    return pl.pallas_call(
        layer_kernel,
        out_shape=[jax.ShapeDtypeStruct(shape, f32) for shape in results],
        in_specs=[pl.BlockSpec(memory_space=pltpu.HBM)] * 13,
        out_specs=[vmem] * 8,
        scratch_shapes=[pltpu.VMEM(a.shape, a.dtype) for a in inputs] + [
            dma((len(inputs),)),
            pltpu.VMEM((pieces, 2) + block, bf16),
            pltpu.VMEM(table, f32), pltpu.VMEM((RING,) + table, f32),
            pltpu.VMEM(state, bf16), pltpu.VMEM((RING,) + state, bf16),
            pltpu.VMEM(state, bf16), pltpu.VMEM((RING,) + state, bf16),
            pltpu.VMEM(query.shape, bf16), pltpu.VMEM(query.shape, bf16),
            pltpu.VMEM(query.shape, bf16),
            pltpu.VMEM(state, f32), pltpu.VMEM(state, bf16), pltpu.VMEM(state, f32),
            pltpu.VMEM((heads, tok_rows, tok_rows), bf16),
            pltpu.VMEM(value.shape, bf16), pltpu.VMEM(value.shape, f32),
            pltpu.VMEM(proj, bf16), pltpu.VMEM(proj, bf16),
            pltpu.VMEM(query.shape, f32), pltpu.VMEM(query.shape, f32),
            pltpu.VMEM((RING, tok_rows, 128), f32),
            pltpu.VMEM(full, bf16), pltpu.VMEM(full, bf16),
            pltpu.VMEM(acts, f32), pltpu.VMEM(acts, f32),
            pltpu.VMEM(acts, bf16), pltpu.VMEM(acts, bf16), pltpu.VMEM(acts, bf16),
            pltpu.VMEM((pieces, RING) + block, bf16), pltpu.VMEM((pieces, RING) + block, bf16),
            pltpu.VMEM((pieces, RING) + block, bf16),
            pltpu.VMEM((pieces, 2, tok_rows // 2, wide), bf16),
            pltpu.VMEM((pieces, 2) + block, bf16),
            pltpu.VMEM((pieces,) + block, bf16), pltpu.VMEM((pieces,) + block, bf16),
            pltpu.VMEM((pieces, 2) + block, bf16),
            dma((2, 3)), dma((2, 3)),
            dma((2, 2, 5)), dma((2, 2, 3)),
            dma((2, 5, 6)), dma((2, 5, 6)),
            dma((2, 4, 5)), dma((2, 4, 5)),
            dma((3,)), dma((3,)), dma((RING, 3)), dma((RING, 3)),
            dma((pieces,)), dma((pieces,)),
            dma((pieces, 2)), dma((pieces, 2)),
            dma((pieces, 4)), dma((pieces, 4)),
            dma((pieces, 2, 2)), dma((pieces, 2, 2)),
            dma((pieces, 2, 2)), dma((pieces, 2, 2)),
        ],
        compiler_params=pltpu.CompilerParams(
            collective_id=0, has_side_effects=True, vmem_limit_bytes=42 << 20
        ),
        name="layer_stage",
    )(*[pltpu.with_memory_space_constraint(a, pltpu.HBM) for a in inputs])


def write_kernel(*refs):
    count = len(refs) // 2
    sems = refs[-1]
    copies = [
        pltpu.make_async_copy(refs[i], refs[count + i], sems.at[i]) for i in range(count)
    ]
    for copy in copies:
        copy.start()
    for copy in copies:
        copy.wait()


def write_out(arrays):
    return pl.pallas_call(
        write_kernel,
        out_shape=[jax.ShapeDtypeStruct(a.shape, a.dtype) for a in arrays],
        in_specs=[pl.BlockSpec(memory_space=pltpu.VMEM)] * len(arrays),
        out_specs=[pl.BlockSpec(memory_space=pltpu.HBM)] * len(arrays),
        scratch_shapes=[pltpu.SemaphoreType.DMA((len(arrays),))],
        compiler_params=pltpu.CompilerParams(vmem_limit_bytes=1 << 20),
        name="write_out",
    )(*arrays)


def ring_local(
    layer_in, out_cot, route_ids, route_probs, group_prob, gate_weight, up_weight,
    down_weight, out_weight, query, key_in, value, decay_logit,
):
    results = write_out(layer_stage(
        layer_in, out_cot, route_ids.T, route_probs.T, group_prob, gate_weight[0], up_weight[0], down_weight[0],
        out_weight, query, key_in, value, decay_logit,
    ))
    return tuple(r[None] for r in results[:3]) + tuple(results[3:])


def solution(mesh):
    in_specs = (
        P("sp", "tp"),
        P("sp", "tp"),
        P("sp", None),
        P("sp", None),
        P("sp"),
        P("sp", "tp", None),
        P("sp", "tp", None),
        P("sp", "tp", None),
        P(None, "tp"),
        P("sp", "tp"),
        P("sp", "tp"),
        P("sp", "tp"),
        P("sp", "tp"),
    )
    out_specs = (
        P("sp", "tp", None),
        P("sp", "tp", None),
        P("sp", "tp", None),
        P("sp", "tp"),
        P("sp", "tp"),
        P("sp", "tp"),
        P("sp", "tp"),
        P("sp", "tp"),
    )
    rows = 4 // mesh.shape["sp"]
    body = ring_local if rows * 4 == 4 and mesh.shape["tp"] == 8 else local
    return jax.shard_map(body, mesh=mesh, in_specs=in_specs, out_specs=out_specs, check_vma=False)
```

```python
import functools
import jax
import jax.numpy as jnp
from jax import lax
from jax.experimental import pallas as pl
from jax.experimental.pallas import tpu as pltpu
from jax.sharding import PartitionSpec as P

DK = 64
DV = 128
BLOCK = 64


decay_temp = 16.0
highest = lax.Precision.HIGH


def prefix(x, axis, join, neutral, backward):
    count = lax.axis_size(axis)
    place = lax.axis_index(axis)
    ahead = count - 1 - place if backward else place
    gathered = jax.tree.map(
        lambda a, kind: lax.all_gather(a.astype(kind), axis),
        x,
        jax.tree.map(lambda a: jnp.bfloat16 if a.dtype == jnp.float32 else a.dtype, x),
    )
    state = jax.tree.map(lambda a, e: jnp.zeros_like(a) + jnp.asarray(e, a.dtype), x, neutral)

    def one(step, state):
        source = count - 1 - step if backward else step
        return join(
            state,
            jax.tree.map(
                lambda a, own: lax.dynamic_index_in_dim(a, source, 0, False).astype(own.dtype),
                gathered,
                x,
            ),
        )

    return lax.fori_loop(0, ahead, one, state)


def combine_spans(earlier, later):
    return (earlier[0] * later[0], later[1] + later[0][..., None] * earlier[1])


def contract_rows(left_mat, right_mat):
    return lax.dot_general(
        left_mat, right_mat, (((0,), (0,)), ((), ())), preferred_element_type=jnp.float32
    )


def contract_cols(left_mat, right_mat):
    return lax.dot_general(
        left_mat, right_mat, (((1,), (1,)), ((), ())), preferred_element_type=jnp.float32
    )


def to_blocks(tensor, head_count):
    rows_here = tensor.shape[0]
    return (
        tensor.astype(jnp.float32)
        .reshape(rows_here // BLOCK, BLOCK, head_count, -1)
        .transpose(2, 0, 1, 3)
    )


def from_blocks(tensor):
    head_count, blocks, _, channels = tensor.shape
    return tensor.transpose(1, 2, 0, 3).reshape(blocks * BLOCK, head_count * channels)


def expert_pass(rows_x, rows_cot, gate_mat, up_mat, down_mat):
    full_x, full_cot = (
        lax.all_gather(rows_x, "tp", axis=1, tiled=True),
        lax.all_gather(rows_cot, "tp", axis=1, tiled=True),
    )
    gate_pre = contract_cols(full_x, gate_mat)
    up_pre = contract_cols(full_x, up_mat)
    sigmoid_gate = jax.nn.sigmoid(gate_pre)
    active = gate_pre * sigmoid_gate
    hidden = (active * up_pre).astype(jnp.bfloat16)
    hidden_cot = contract_cols(full_cot, down_mat)
    up_cot = (hidden_cot * active).astype(jnp.bfloat16)
    gate_cot = (
        hidden_cot * up_pre * sigmoid_gate * (1.0 + gate_pre * (1.0 - sigmoid_gate))
    ).astype(jnp.bfloat16)
    down_g = contract_rows(hidden, full_cot)
    gate_g = contract_rows(gate_cot, full_x)
    up_g = contract_rows(up_cot, full_x)
    dims = (((0,), (1,)), ((), ()))
    first_part = lax.dot_general(gate_mat, gate_cot, dims, preferred_element_type=jnp.float32)
    back_terms = lax.psum_scatter(
        (
            first_part + lax.dot_general(up_mat, up_cot, dims, preferred_element_type=jnp.float32)
        ).astype(jnp.bfloat16),
        "tp",
        scatter_dimension=0,
        tiled=True,
    ).astype(jnp.float32)
    return (gate_g, up_g, down_g, back_terms)


def local(
    layer_in,
    out_cot,
    route_ids,
    route_probs,
    group_prob,
    gate_weight,
    up_weight,
    down_weight,
    out_weight,
    query,
    key_in,
    value,
    decay_logit,
):
    tok_rows = layer_in.shape[0]
    local_cols = layer_in.shape[1]
    experts_all = lax.axis_size("sp")
    capacity = 4 * tok_rows // experts_all
    route_weight = group_prob[:, None] * route_probs / jnp.sum(route_probs, axis=1, keepdims=True)
    chosen = (route_ids[:, :, None] == jnp.arange(experts_all, dtype=jnp.int32)).astype(jnp.int32)
    running = jnp.cumsum(chosen.reshape(2 * tok_rows, experts_all), axis=0).reshape(
        tok_rows, 2, experts_all
    )
    position = jnp.sum((running - 1) * chosen, axis=2)
    slot_ids = route_ids * capacity + position
    matches = (
        slot_ids[None, :, :] == jnp.arange(experts_all * capacity, dtype=jnp.int32)[:, None, None]
    )
    select_x = jnp.any(matches, axis=2).astype(jnp.float32)
    select_cot = jnp.sum(jnp.where(matches, route_weight[None], 0.0), axis=2)
    send_x = jnp.dot(
        select_x.astype(jnp.bfloat16), layer_in, preferred_element_type=jnp.float32
    ).astype(jnp.bfloat16)
    send_cot = jnp.dot(select_cot, out_cot.astype(jnp.float32), precision=highest).astype(
        jnp.bfloat16
    )
    send_x = send_x.reshape(experts_all, capacity, local_cols)
    send_cot = send_cot.reshape(experts_all, capacity, local_cols)
    recv_x, recv_cot = (
        lax.all_to_all(send_x, "sp", split_axis=0, concat_axis=0, tiled=True),
        lax.all_to_all(send_cot, "sp", split_axis=0, concat_axis=0, tiled=True),
    )
    head_dev = query.shape[1] // DK
    scaled_query = to_blocks(query, head_dev) * DK ** (-0.5)
    key_blk = to_blocks(key_in, head_dev)
    value_blk = to_blocks(value, head_dev)
    logit_blk = to_blocks(decay_logit, head_dev)
    cumulative = jnp.cumsum(jax.nn.log_sigmoid(logit_blk) / decay_temp, axis=2)
    span_log = cumulative[:, :, -1:, :]
    growth = jnp.exp(cumulative)
    shrink = jnp.exp(-cumulative)
    to_end = jnp.exp(span_log - cumulative)
    query_decayed = scaled_query * growth
    key_back = key_blk * shrink
    key_to_end = key_blk * to_end
    causal = jnp.tril(jnp.ones((BLOCK, BLOCK), dtype=bool))
    scores = jnp.where(
        causal, jnp.einsum("hncd,hnsd->hncs", query_decayed, key_back, precision=highest), 0.0
    )
    within = jnp.einsum("hncs,hnsv->hncv", scores, value_blk, precision=highest)
    block_decay = jnp.moveaxis(jnp.exp(span_log[:, :, 0, :]), 1, 0)
    block_update = jnp.moveaxis(
        jnp.einsum("hncd,hncv->hndv", key_to_end, value_blk, precision=highest), 1, 0
    )
    identity_pair = (
        jnp.ones((head_dev, DK), jnp.float32),
        jnp.zeros((head_dev, DK, DV), jnp.float32),
    )

    def advance(carry_pair, inputs):
        return (combine_spans(carry_pair, inputs), carry_pair)

    span_total, before_pairs = lax.scan(advance, identity_pair, (block_decay, block_update))
    entry_pair = prefix(span_total, "sp", combine_spans, identity_pair, False)
    entry_state = entry_pair[1]
    decay_before = jnp.moveaxis(before_pairs[0], 0, 1)
    block_state = decay_before[..., None] * entry_state[:, None] + jnp.moveaxis(
        before_pairs[1], 0, 1
    )
    span_end = span_total[0][..., None] * entry_state + span_total[1]
    outputs = within + jnp.einsum("hncd,hndv->hncv", query_decayed, block_state, precision=highest)
    mixer_out = from_blocks(outputs).astype(jnp.bfloat16)
    gate_mat, up_mat, down_mat = (gate_weight[0], up_weight[0], down_weight[0])
    gate_g, up_g, down_g, back_flat = expert_pass(
        recv_x.reshape(-1, local_cols), recv_cot.reshape(-1, local_cols), gate_mat, up_mat, down_mat
    )
    back_terms = back_flat.reshape(local_cols, experts_all, capacity)
    returned = lax.all_to_all(
        back_terms.astype(jnp.bfloat16), "sp", split_axis=1, concat_axis=1, tiled=True
    ).astype(back_terms.dtype)
    returned = returned.reshape(local_cols, experts_all * capacity)
    routed_sum = lax.dot_general(
        select_x,
        returned,
        (((0,), (1,)), ((), ())),
        precision=highest,
        preferred_element_type=jnp.float32,
    )
    mixed_cot = (out_cot.astype(jnp.float32) + routed_sum).astype(jnp.bfloat16)
    full_cot = lax.all_gather(mixed_cot, "tp", axis=1, tiled=True)
    mixer_cot = jnp.dot(full_cot, out_weight, preferred_element_type=jnp.float32)
    proj_grad = lax.psum_scatter(
        contract_rows(full_cot, mixer_out).astype(jnp.bfloat16),
        "sp",
        scatter_dimension=0,
        tiled=True,
    ).astype(jnp.float32)
    cot_blk = to_blocks(mixer_cot, head_dev)
    block_future = jnp.moveaxis(
        jnp.einsum("hncd,hncv->hndv", query_decayed, cot_blk, precision=highest), 1, 0
    )

    def retreat(carry_pair, inputs):
        return (combine_spans(carry_pair, inputs), carry_pair)

    span_back, after_pairs = lax.scan(
        retreat, identity_pair, (block_decay, block_future), reverse=True
    )
    beyond_pair = prefix(span_back, "sp", combine_spans, identity_pair, True)
    future_state = beyond_pair[1]
    decay_after = jnp.moveaxis(after_pairs[0], 0, 1)
    block_future_state = decay_after[..., None] * future_state[:, None] + jnp.moveaxis(
        after_pairs[1], 0, 1
    )
    cot_values = jnp.where(
        causal, jnp.einsum("hncv,hnsv->hncs", cot_blk, value_blk, precision=highest), 0.0
    )
    query_scaled_grad = growth * (
        jnp.einsum("hncv,hndv->hncd", cot_blk, block_state, precision=highest)
        + jnp.einsum("hncs,hnsd->hncd", cot_values, key_back, precision=highest)
    )
    key_part = shrink * jnp.einsum("hncs,hncd->hnsd", cot_values, query_decayed, precision=highest)
    key_grad = key_part + to_end * jnp.einsum(
        "hnsv,hndv->hnsd", value_blk, block_future_state, precision=highest
    )
    value_grad = jnp.einsum("hncs,hncv->hnsv", scores, cot_blk, precision=highest) + jnp.einsum(
        "hnsd,hndv->hnsv", key_to_end, block_future_state, precision=highest
    )
    decay_terms = (scaled_query * query_scaled_grad - key_blk * key_grad).reshape(
        head_dev, tok_rows, DK
    )
    tail_sum = jnp.flip(jnp.cumsum(jnp.flip(decay_terms, 1), axis=1), 1)
    beyond_term = jnp.sum(future_state * span_end, axis=2)
    log_grad = tail_sum + beyond_term[:, None, :]
    logit_flat = logit_blk.reshape(head_dev, tok_rows, DK)
    logit_grad = (
        (log_grad * jax.nn.sigmoid(-logit_flat) / decay_temp)
        .transpose(1, 0, 2)
        .reshape(tok_rows, head_dev * DK)
    )
    query_grad = from_blocks(query_scaled_grad * DK ** (-0.5))
    return (
        gate_g[None],
        up_g[None],
        down_g[None],
        proj_grad,
        query_grad,
        from_blocks(key_grad),
        from_blocks(value_grad),
        logit_grad,
    )


RING = 4
EXPERT_CUT = 5
PIECES = 8
GATHER_ORDER = (
    ("zs", 0, 0),
    ("rs", 1, 4),
    ("rs", 0, 4),
    ("zs", 1, 0),
    ("rs", 0, 0),
    ("rf", 0, 4, 1),
    ("rf", 1, 4, 1),
    ("prep",),
    ("rf", 1, 4, 0),
    ("rf", 0, 4, 0),
    ("rn", 0, 4),
    ("zr", 0, 0, 1),
    ("rf", 0, 0, 1),
    ("rs", 1, 0),
    ("rn", 1, 4),
    ("zr", 0, 0, 2),
    ("zr", 1, 0, 1),
    ("ro", 1, 4),
    ("ro", 0, 4),
    ("rf", 0, 1, 0),
    ("zr", 0, 0, 3),
    ("rf", 0, 1, 1),
    ("zr", 1, 1, 1),
    ("zr", 1, 0, 2),
    ("rf", 1, 0, 1),
    ("zr", 0, 1, 2),
    ("rn", 0, 1),
    ("rf", 1, 1, 0),
    ("rf", 0, 0, 0),
    ("rf", 0, 2, 0),
    ("mixf",),
    ("rf", 1, 1, 1),
    ("rf", 0, 2, 1),
    ("rn", 0, 0),
    ("rn", 1, 1),
    ("zr", 1, 1, 3),
    ("fx", 0),
    ("zr", 0, 1, 1),
    ("rf", 1, 0, 0),
    ("rn", 1, 0),
    ("rf", 0, 3, 1),
    ("rf", 0, 3, 0),
    ("rn", 0, 2),
    ("rn", 0, 3),
    ("zr", 1, 0, 3),
    ("fx", 1),
    ("rf", 1, 2, 1),
    ("rf", 1, 2, 0),
    ("zr", 0, 1, 3),
    ("fx", 3),
    ("ro", 0, 1),
    ("rn", 1, 2),
    ("sy", 0),
    ("zr", 1, 1, 2),
    ("fx", 4),
    ("ro", 0, 3),
    ("ro", 0, 0),
    ("rf", 1, 3, 0),
    ("rf", 1, 3, 1),
    ("ro", 0, 2),
    ("fx", 2),
    ("rn", 1, 3),
    ("sy", 4),
    ("ro", 1, 1),
    ("ro", 1, 0),
    ("ro", 1, 2),
    ("sy", 3),
    ("sy", 1),
)
REDUCE_ORDER = (
    ("ptb", 0),
    ("ro", 1, 3),
    ("sy", 2),
    ("pto", 0),
    ("opb", 0),
    ("g", 11),
    ("pto", 1),
    ("ptb", 1),
    ("opo", 0),
    ("pt", 2),
    ("opo", 1),
    ("opb", 1),
    ("rl", 0, 1),
    ("rl", 2, 0),
    ("rl", 1, 0),
    ("rl", 1, 1),
    ("rl", 2, 1),
    ("op", 2),
    ("g", 6),
    ("pt", 3),
    ("to", 2, 0),
    ("to", 1, 0),
    ("g", 7),
    ("to", 1, 1),
    ("g", 9),
    ("rl", 4, 0),
    ("rl", 3, 1),
    ("g", 0),
    ("rl", 0, 0),
    ("rl", 4, 1),
    ("g", 1),
    ("to", 0, 1),
    ("rl", 5, 0),
    ("mi", 1, 0),
    ("rl", 3, 0),
    ("mi", 2, 0),
    ("to", 2, 1),
    ("rl", 5, 1),
    ("op", 3),
    ("to", 4, 0),
    ("mi", 0, 1),
    ("to", 0, 0),
    ("mi", 1, 1),
    ("to", 3, 1),
    ("to", 5, 0),
    ("lt", 1, 0),
    ("to", 3, 0),
    ("g", 10),
    ("rl", 6, 1),
    ("mi", 4, 0),
    ("rl", 6, 0),
    ("to", 4, 1),
    ("lt", 2, 0),
    ("mi", 2, 1),
    ("mi", 0, 0),
    ("g", 5),
    ("to", 5, 1),
    ("rl", 7, 1),
    ("lt", 0, 1),
    ("mi", 3, 1),
    ("rl", 7, 0),
    ("g", 3),
    ("to", 6, 1),
    ("to", 6, 0),
    ("lt", 1, 1),
    ("g", 2),
    ("mi", 3, 0),
    ("lt", 4, 0),
    ("mi", 4, 1),
    ("to", 7, 1),
    ("to", 7, 0),
    ("lt", 0, 0),
    ("lt", 2, 1),
    ("mi", 5, 0),
    ("lt", 3, 1),
    ("gd", 0),
    ("gd", 1),
    ("mi", 5, 1),
    ("pj", 0),
    ("gd", 2),
    ("lt", 3, 0),
    ("mi", 6, 1),
    ("lt", 4, 1),
    ("mi", 6, 0),
    ("gd", 3),
    ("gd", 4),
    ("lt", 5, 0),
    ("pj", 1),
    ("lt", 5, 1),
    ("mi", 7, 1),
    ("mi", 7, 0),
    ("lt", 6, 1),
    ("gd", 5),
    ("g", 8),
    ("lt", 6, 0),
    ("pj", 2),
    ("lt", 7, 1),
    ("lt", 7, 0),
    ("gd", 6),
    ("gd", 7),
    ("mb",),
    ("pj", 3),
    ("g", 4),
    ("mb2",),
    ("mb3",),
    ("mf",),
)


def ring_place(index):
    return index + (index // 2) * (1 - 2 * (index % 2))


def remote(source, target, send_sem, recv_sem, device):
    return pltpu.make_async_remote_copy(
        src_ref=source,
        dst_ref=target,
        send_sem=send_sem,
        recv_sem=recv_sem,
        device_id=device,
        device_id_type=pl.DeviceIdType.MESH,
    )


def greet(devices):
    barrier = pltpu.get_barrier_semaphore()
    for device in devices:
        pl.semaphore_signal(
            barrier, inc=1, device_id=device, device_id_type=pl.DeviceIdType.MESH
        )
    pl.semaphore_wait(barrier, len(devices))


def arrived(sem, region):
    pltpu.make_async_copy(region, region, sem).wait()


class Place:
    def __init__(self):
        self.sp, self.tp = lax.axis_index("sp"), lax.axis_index("tp")
        self.z, self.core = self.tp // 2, self.tp % 2
        ring = ring_place(self.sp)
        self.at = [ring_place((ring + step) % RING) for step in range(RING)]
        self.right, self.across, self.left = [(self.at[s], self.tp) for s in (1, 2, 3)]
        self.pair = (self.sp, 2 * self.z + 1 - self.core)
        self.near = (self.sp, 2 * (self.z + 1 - 2 * (self.z % 2)) + self.core)
        self.far = (self.sp, 2 * (RING - 1 - self.z) + self.core)
        upper = self.z // 2
        folded = self.z + upper * (RING - 1 - 2 * self.z)
        self.inner = folded == 1
        self.end = folded == 0
        order = [folded, 1 - folded, 2, 3]
        self.slot = [o + upper * (RING - 1 - 2 * o) for o in order]


def layer_kernel(
    x_far, cot_far, ids_far, probs_far, group_far, gate_far, up_far, down_far, out_far,
    query_far, key_far, value_far, logit_far,
    gate_out, up_out, down_out, proj_out, query_out, key_out, value_out, logit_out,
    x_ref, cot_ref, ids_ref, probs_ref, group_ref, gate_ref, up_ref, down_ref, out_ref,
    query_ref, key_ref, value_ref, logit_ref, load_sem,
    mixed, small_buf, small_out, state_buf, state_out, future_buf, future_out,
    decayed, key_back, key_end, state_own, entry, span_end, scores, mixer_out, mixer_cot,
    proj_to, proj_from, summed, terms, weights,
    x_all, cot_all, gate_pre, up_pre, hidden, gate_cot, up_cot,
    pair_to, pair_from, parts, first_in, second_in, total, half_total, z_in,
    tiny_send, tiny_recv, zs, zr, ps, pr, qs, qr,
    fs, fr, js, jr, bs, br, r1s, r1r, r2s, r2r, zts, ztr, ms, mr,
):
    here = Place()
    loads = [
        pltpu.make_async_copy(far, near, load_sem.at[i])
        for i, (far, near) in enumerate((
            (x_far, x_ref), (cot_far, cot_ref), (ids_far, ids_ref), (probs_far, probs_ref),
            (group_far, group_ref), (query_far, query_ref), (key_far, key_ref),
            (value_far, value_ref), (logit_far, logit_ref), (gate_far, gate_ref),
            (up_far, up_ref), (down_far, down_ref), (out_far, out_ref),
        ))
    ]
    for copy in loads:
        copy.start()
    tok_rows, width = x_ref.shape
    lead = tok_rows * 4 // EXPERT_CUT
    tail = tok_rows - lead
    ins, alls = (x_ref, cot_ref), (x_all, cot_all)
    greet([here.right, here.across, here.left, here.near, here.far, here.pair])
    for copy in loads[:2]:
        copy.wait()
    plain, guarded = [], []

    def go(source, target, send_sem, recv_sem, device):
        copy = remote(source, target, send_sem, recv_sem, device)
        copy.start()
        plain.append(copy)

    def go_if(cond, source, target, send_sem, recv_sem, device):
        copy = remote(source, target, send_sem, recv_sem, device)

        @pl.when(cond)
        def _():
            copy.start()

        guarded.append((cond, copy))

    def cols(slot, core):
        return pl.ds(pl.multiple_of((2 * here.slot[slot] + core) * width, width), width)

    def piece(a, part, slot, core=None):
        core = here.core if core is None else core
        if part == 0:
            return alls[a].at[here.sp, pl.ds(0, lead), cols(slot, core)]
        return alls[a].at[:, pl.ds(lead, tail), cols(slot, core)]

    def own_rows(a, start, count):
        return ins[a].at[pl.ds(start, count), :]

    def z_start(a, part):
        source = own_rows(a, 0, lead) if part == 0 else piece(a, 1, 0)
        target = piece(a, part, 0)
        go(source, target, zs.at[a, part, 0], zr.at[a, part, 0], here.near)
        go_if(here.inner, source, target, zs.at[a, part, 1], zr.at[a, part, 1], here.far)

    def z_relay(a, part, slot):
        region = piece(a, part, slot)
        arrived(zr.at[a, part, slot - 1], region)
        if slot == 1:
            go_if(here.inner, region, region, zs.at[a, part, 2], zr.at[a, part, 2], here.far)
        else:
            go_if(
                here.inner, region, region, zs.at[a, part, slot + 1], zr.at[a, part, slot - 1],
                here.near,
            )
        if part == 0:
            pair_send(a, slot, 0)
            ring_send(a, (slot, 0))
        else:
            go(region, region, qs.at[a, slot, 4], qr.at[a, slot, 4], here.pair)

    def bounds(part, h):
        start, count = (0, lead) if part == 0 else (lead, tail)
        return start + h * (count // 2), count // 2

    def ring_region(a, unit, step, h):
        slot, part = unit
        start, count = bounds(part, h)
        return alls[a].at[here.at[step], pl.ds(start, count), cols(slot, here.core)]

    def number(unit):
        return unit[0] + 4 * unit[1]

    def ring_send(a, unit):
        slot, part = unit
        n = number(unit)
        for i, (h, device) in enumerate(
            ((0, here.right), (1, here.right), (0, here.left), (1, here.left))
        ):
            start, count = bounds(part, h)
            source = own_rows(a, start, count) if slot == 0 else ring_region(a, unit, 0, h)
            copy = remote(source, ring_region(a, unit, 0, h), ps.at[a, n, i], pr.at[a, n, i], device)
            plain.append(copy)
        right0, right1, left0, left1 = plain[-4:]
        for copy in (right0, left1, right1, left0):
            copy.start()

    def ring_forward(a, unit, h):
        n = number(unit)
        region = ring_region(a, unit, (3, 1)[h], h)
        arrived(pr.at[a, n, 3 * h], region)
        go(region, region, ps.at[a, n, 4 + h], pr.at[a, n, 4 + h], (here.right, here.left)[h])

    def ring_near(a, unit):
        n = number(unit)
        arrived(pr.at[a, n, 1], ring_region(a, unit, 3, 1))
        arrived(pr.at[a, n, 2], ring_region(a, unit, 1, 0))
        if unit[1] == 0:
            pair_send(a, unit[0], 1)
            pair_send(a, unit[0], 3)

    def ring_across(a, unit):
        n = number(unit)
        arrived(pr.at[a, n, 4], ring_region(a, unit, 2, 0))
        arrived(pr.at[a, n, 5], ring_region(a, unit, 2, 1))
        if unit[1] == 0:
            pair_send(a, unit[0], 2)
        else:
            z_start(a, 1)
            region = piece(a, 1, 0)
            go(region, region, qs.at[a, 0, 4], qr.at[a, 0, 4], here.pair)

    def pair_region(a, slot, step, core):
        return alls[a].at[here.at[step], pl.ds(0, lead), cols(slot, core)]

    def pair_send(a, slot, step):
        region = pair_region(a, slot, step, here.core)
        source = own_rows(a, 0, lead) if slot == 0 and step == 0 else region
        go(source, region, qs.at[a, slot, step], qr.at[a, slot, step], here.pair)

    def pair_wait(a, step):
        for slot in range(RING):
            if step < 4:
                arrived(qr.at[a, slot, step], pair_region(a, slot, step, 1 - here.core))
            else:
                arrived(qr.at[a, slot, 4], piece(a, 1, slot, 1 - here.core))

    bf16, f32 = jnp.bfloat16, jnp.float32
    key_cols = query_ref.shape[1]
    heads = key_cols // DK
    lane = lax.broadcasted_iota(jnp.int32, (1, key_cols), 1) // DK
    row = lax.broadcasted_iota(jnp.int32, (key_cols, 1), 0) // DK

    def dot(left, right, left_dim=1, right_dim=0, precision=None):
        return lax.dot_general(
            left, right, (((left_dim,), (right_dim,)), ((), ())),
            precision=precision, preferred_element_type=f32,
        )

    def two(value):
        high = value.astype(bf16)
        return high, (value - high.astype(f32)).astype(bf16)

    def triangle():
        return lax.broadcasted_iota(jnp.int32, (tok_rows, tok_rows), 0) >= (
            lax.broadcasted_iota(jnp.int32, (tok_rows, tok_rows), 1)
        )

    def only(value, h):
        return jnp.where(lane == h, value, jnp.zeros_like(value))

    def join(parts_of, which):
        joined = parts_of[0]
        for h in range(1, heads):
            joined = jnp.where(which == h, parts_of[h], joined)
        return joined

    def head_cols(h):
        return pl.ds(h * DV, DV)

    def log_decay(logit):
        return -(jnp.maximum(-logit, 0.0) + jnp.log(1.0 + jnp.exp(-jnp.abs(logit)))) / decay_temp

    def column(s):
        pick = (
            lax.broadcasted_iota(jnp.int32, (small_buf.shape[0], DV), 0) == RING
        ).astype(f32)
        return dot(
            small_out[s, :, pl.ds(0, key_cols)], pick, 0, 0, lax.Precision.HIGHEST
        )

    def mix_prepare():
        for copy in loads[2:]:
            copy.wait()
        ones = triangle().astype(bf16)
        high, low = two(log_decay(logit_ref[...].astype(f32)))
        cumulative = dot(ones, high) + dot(ones, low)
        summed[...] = cumulative
        last = cumulative[tok_rows - 1 : tok_rows, :]
        keys = key_ref[...].astype(f32)
        decayed[...] = (
            query_ref[...].astype(f32) * DK ** (-0.5) * jnp.exp(cumulative)
        ).astype(bf16)
        key_back[...] = (keys * jnp.exp(-cumulative)).astype(bf16)
        ends = (keys * jnp.exp(last - cumulative)).astype(bf16)
        key_end[...] = ends
        state = join([dot(ends, value_ref[:, head_cols(h)], 0, 0) for h in range(heads)], row)
        state_own[...] = state
        state_buf[...] = state.astype(bf16)
        share = group_ref[...].reshape(1, tok_rows) / (probs_ref[0:1, :] + probs_ref[1:2, :])
        expert = lax.broadcasted_iota(jnp.int32, (small_buf.shape[0], tok_rows), 0)
        small_buf[...] = jnp.zeros_like(small_buf)
        small_buf[:, pl.ds(0, tok_rows)] = sum(
            jnp.where(ids_ref[j : j + 1, :] == expert, share * probs_ref[j : j + 1, :], 0.0)
            for j in range(2)
        )
        small_buf[RING : RING + 1, pl.ds(0, key_cols)] = jnp.exp(last)
        small_out[here.sp] = small_buf[...]
        state_out[here.sp] = state_buf[...]
        for i, (buf, out) in enumerate(((small_buf, small_out), (state_buf, state_out))):
            for step, device in ((1, here.right), (3, here.left), (2, here.across)):
                go(
                    buf, out.at[here.sp], tiny_send.at[i, step - 1], tiny_recv.at[i, 3 - step],
                    device,
                )

    def mix_forward():
        for step in (1, 2, 3):
            arrived(tiny_recv.at[0, step - 1], small_out.at[here.at[step]])
            arrived(tiny_recv.at[1, step - 1], state_out.at[here.at[step]])
        state = jnp.zeros((key_cols, DV), f32)
        for s in range(RING - 1):
            later = state * column(s) + state_out[s].astype(f32)
            state = jnp.where(here.sp > s, later, state)
        entry[...] = state.astype(bf16)
        mine = (
            lax.broadcasted_iota(jnp.int32, (small_buf.shape[0], 128), 0) == here.sp
        ).astype(f32)
        for s in range(RING):
            weights[s] = dot(small_out[s], mine, 0, 0, lax.Precision.HIGHEST)[:tok_rows]
        span_end[...] = state * column(here.sp) + state_own[...]
        keep = triangle()
        for h in range(heads):
            mine = only(decayed[...], h)
            score = jnp.where(keep, dot(mine, key_back[...], 1, 1), 0.0).astype(bf16)
            scores[h] = score
            mixer_out[:, head_cols(h)] = (
                dot(score, value_ref[:, head_cols(h)]) + dot(mine, entry[...])
            ).astype(bf16)

    def mix_backward():
        cot = [mixer_cot[:, head_cols(h)].astype(bf16) for h in range(heads)]
        future = join([dot(decayed[...], cot[h], 0, 0) for h in range(heads)], row)
        future_buf[...] = future.astype(bf16)
        for step, device in ((1, here.right), (3, here.left), (2, here.across)):
            go(
                future_buf, future_out.at[here.sp], fs.at[step - 1], fr.at[3 - step], device
            )

    held = {}

    def mix_inner():
        keep = triangle()
        cot = [mixer_cot[:, head_cols(h)].astype(bf16) for h in range(heads)]
        pairs = [
            jnp.where(keep, dot(cot[h], value_ref[:, head_cols(h)], 1, 1), 0.0).astype(bf16)
            for h in range(heads)
        ]
        inner = join(
            [dot(cot[h], entry[...], 1, 1) + dot(pairs[h], key_back[...]) for h in range(heads)],
            lane,
        )
        key_inner = join([dot(pairs[h], decayed[...], 0, 0) for h in range(heads)], lane)
        query_out[...] = jnp.exp(summed[...]) * inner * DK ** (-0.5)
        key_out[...] = jnp.exp(-summed[...]) * key_inner
        terms[...] = (
            decayed[...].astype(f32) * inner - key_back[...].astype(f32) * key_inner
        )
        for h in range(heads):
            value_out[:, head_cols(h)] = dot(scores[h], cot[h], 0, 0)

    def mix_outer():
        for step in (1, 2, 3):
            arrived(fr.at[step - 1], future_out.at[here.at[step]])
        state = jnp.zeros((key_cols, DV), f32)
        for s in range(RING - 1, 0, -1):
            earlier = state * column(s) + future_out[s].astype(f32)
            state = jnp.where(here.sp < s, earlier, state)
        ahead = state.astype(bf16)
        key_outer = join(
            [dot(value_ref[:, head_cols(h)], ahead, 1, 1) for h in range(heads)], lane
        )
        last = summed[tok_rows - 1 : tok_rows, :]
        key_out[...] += jnp.exp(last - summed[...]) * key_outer
        for h in range(heads):
            value_out[:, head_cols(h)] += dot(only(key_end[...], h), ahead)
        high, low = two(terms[...] - key_end[...].astype(f32) * key_outer)
        ones = triangle().astype(bf16)
        tail_sum = dot(ones, high, 0, 0) + dot(ones, low, 0, 0)
        beyond = dot(
            jnp.ones((8, DV), f32), state * span_end[...], 1, 1, lax.Precision.HIGHEST
        )[0:1, :]
        logit_out[...] = (tail_sum + beyond) / (
            decay_temp * (1.0 + jnp.exp(logit_ref[...].astype(f32)))
        )

    def mix_finish():
        for m in range(RING):
            result = proj_to[m, here.sp].astype(f32)
            for step in (1, 3, 2):
                arrived(jr.at[m, step - 1], proj_from.at[m, here.at[step]])
                result = result + proj_from[m, here.at[step]].astype(f32)
            proj_out[pl.ds(m * atom, atom), :] = result

    def block_of(ref, s):
        if s is None:
            return ref[:, pl.ds(lead, tail), :].reshape(RING * tail, ref.shape[2])
        return ref[s, pl.ds(0, lead), :]

    def keep_block(ref, s, value):
        if s is None:
            ref[:, pl.ds(lead, tail), :] = value.reshape(RING, tail, ref.shape[2])
        else:
            ref[s, pl.ds(0, lead), :] = value

    def forward_rows(s):
        block = block_of(x_all, s)
        keep_block(gate_pre, s, contract_cols(block, gate_ref[...]))
        keep_block(up_pre, s, contract_cols(block, up_ref[...]))

    def second_rows(s):
        weight = jnp.concatenate([block_of(weights, s)] * (width // 128), axis=1)
        hidden_cot = contract_cols(block_of(cot_all, s), down_ref[...]) * weight
        gp, upp = block_of(gate_pre, s), block_of(up_pre, s)
        sig = 1.0 / (1.0 + jnp.exp(-gp))
        active = gp * sig
        keep_block(hidden, s, (active * upp * weight).astype(jnp.bfloat16))
        keep_block(up_cot, s, (hidden_cot * active).astype(jnp.bfloat16))
        keep_block(
            gate_cot, s,
            (hidden_cot * upp * sig * (1.0 + gp * (1.0 - sig))).astype(jnp.bfloat16),
        )

    def rows_of(a, step, work):
        pair_wait(a, step)
        work(here.at[step] if step < RING else None)

    def own_start(a):
        ring_send(a, (0, 0))
        pair_send(a, 0, 0)

    gather_steps = {
        "zs": z_start,
        "rs": lambda a, n: own_start(a) if n == 0 else ring_send(a, (0, 1)),
        "zr": z_relay,
        "rf": lambda a, n, h: ring_forward(a, (n % 4, n // 4), h),
        "rn": lambda a, n: ring_near(a, (n % 4, n // 4)),
        "ro": lambda a, n: ring_across(a, (n % 4, n // 4)),
        "prep": mix_prepare,
        "mixf": mix_forward,
        "fx": lambda i: rows_of(0, i, forward_rows),
        "sy": lambda i: rows_of(1, i, second_rows),
    }
    for a in range(2):
        alls[a][here.sp, :, cols(0, here.core)] = ins[a][...]
    pieces, wide = parts.shape[0], parts.shape[3]
    split = tok_rows // 2
    span = gate_ref.shape[1] // RING
    atom = span // RING
    per = 2 * atom // wide

    def atoms(k, core):
        for i in range(wide // atom):
            target = 2 * core + (k % per) + i
            yield pl.ds(pl.multiple_of(target * span + (k // per) * atom, atom), atom)

    def columns(ref, k, core):
        return jnp.concatenate([ref[:, c] for c in atoms(k, core)], axis=1)

    top, bottom = pl.ds(0, split), pl.ds(split, split)

    def partial(m, core, steps):
        weight_of = [
            jnp.concatenate([columns(ref, m * per + i, core) for i in range(per)], axis=1)
            for ref in (gate_ref, up_ref)
        ]
        sides = (gate_cot, up_cot)
        if len(steps) == RING:
            rows = RING * tok_rows
            both = sum(
                jnp.dot(c[...].reshape(rows, width), w, preferred_element_type=jnp.float32)
                for c, w in zip(sides, weight_of)
            )
            for i in range(per):
                part = both[:, i * wide : (i + 1) * wide]
                yield m * per + i, slice(None), part.reshape(RING, tok_rows, wide)
            return
        for step in steps:
            s = here.at[step]
            both = sum(
                jnp.dot(c[s], w, preferred_element_type=jnp.float32)
                for c, w in zip(sides, weight_of)
            )
            for i in range(per):
                yield m * per + i, s, both[:, i * wide : (i + 1) * wide]

    everything, beside, others = (2, 1, 3, 0), (1, 3), (2, 0)

    def pair_part(m, steps):
        for k, s, part in partial(m, 1 - here.core, steps):
            pair_to[k, s] = part.astype(jnp.bfloat16)
        for k in range(m * per, (m + 1) * per):
            for step in steps:
                s = here.at[step]
                go(
                    pair_to.at[k, s], pair_from.at[k, s], bs.at[k, step], br.at[k, step], here.pair
                )

    def own_part(m, steps):
        for k in range(m * per, (m + 1) * per):
            for step in steps:
                arrived(br.at[k, step], pair_from.at[k, here.at[step]])
        for k, s, part in partial(m, here.core, steps):
            parts[k, s] = (part + pair_from[k, s].astype(jnp.float32)).astype(jnp.bfloat16)
        for k in range(m * per, (m + 1) * per):
            right, across, left = [parts.at[k, here.at[i]] for i in (1, 2, 3)]
            if 2 in steps:
                go(across.at[top], first_in.at[k, 0], r1s.at[k, 0], r1r.at[k, 0], here.right)
                go(across.at[bottom], first_in.at[k, 1], r1s.at[k, 1], r1r.at[k, 1], here.left)
            if 1 in steps:
                go(
                    right.at[bottom], second_in.at[k, 0, bottom], r2s.at[k, 0], r2r.at[k, 0],
                    here.right,
                )
            if 3 in steps:
                go(left.at[top], second_in.at[k, 1, top], r2s.at[k, 1], r2r.at[k, 1], here.left)

    def add_to(ref, other):
        ref[...] = (ref[...].astype(jnp.float32) + other.astype(jnp.float32)).astype(jnp.bfloat16)

    def ring_relay(k, h):
        step, rows, device = ((1, top, here.right), (3, bottom, here.left))[h]
        arrived(r1r.at[k, h], first_in.at[k, h])
        mine = parts.at[k, here.at[step]].at[rows]
        add_to(mine, first_in[k, h])
        go(
            mine, second_in.at[k, h, rows],
            r2s.at[k, 2 + h], r2r.at[k, 2 + h], device,
        )

    halves = (top, bottom)

    def ring_total(k, h):
        rows = halves[h]
        own_sem, sum_sem = ((1, 2), (0, 3))[h]
        own_from, sum_from = ((1, 0), (0, 1))[h]
        arrived(r2r.at[k, own_sem], second_in.at[k, own_from, rows])
        arrived(r2r.at[k, sum_sem], second_in.at[k, sum_from, rows])
        total[k, rows] = (
            parts[k, here.sp, rows].astype(jnp.float32)
            + second_in[k, 0, rows].astype(jnp.float32)
            + second_in[k, 1, rows].astype(jnp.float32)
        ).astype(jnp.bfloat16)
        go_if(
            here.end, total.at[k, rows], z_in.at[k, 0, rows], zts.at[k, h, 0], ztr.at[k, h, 0],
            here.near,
        )

    def line_middle(k, h):
        rows = halves[h]
        copy = remote(
            half_total.at[k, rows], z_in.at[k, 1, rows], zts.at[k, h, 1], ztr.at[k, h, 1], here.far
        )

        @pl.when(here.inner)
        def _():
            arrived(ztr.at[k, h, 0], z_in.at[k, 0, rows])
            half_total[k, rows] = (
                total[k, rows].astype(jnp.float32) + z_in[k, 0, rows].astype(jnp.float32)
            ).astype(jnp.bfloat16)
            copy.start()

        guarded.append((here.inner, copy))

    def line_total(k, h):
        rows = halves[h]
        region = mixed.at[k, here.core, rows]
        copy = remote(region, region, ms.at[k, h, 0], mr.at[k, h, 0], here.near)

        @pl.when(here.inner)
        def _():
            arrived(ztr.at[k, h, 1], z_in.at[k, 1, rows])
            mixed[k, here.core, rows] = (
                columns(cot_all.at[here.sp, rows], k, here.core).astype(jnp.float32)
                + (
                    half_total[k, rows].astype(jnp.float32)
                    + z_in[k, 1, rows].astype(jnp.float32)
                )
            ).astype(jnp.bfloat16)
            copy.start()

        guarded.append((here.inner, copy))

        @pl.when(here.end)
        def _():
            arrived(mr.at[k, h, 0], region)

        go(region, region, ms.at[k, h, 1], mr.at[k, h, 1], here.pair)

    features = gate_ref.shape[1]
    block_cols = 2 * width

    def weight_grad(n):
        which, j = n % 3, n // 3
        left, right, out = (
            (gate_cot, x_all, gate_out), (up_cot, x_all, up_out), (hidden, cot_all, down_out)
        )[which]
        c = pl.ds(j * block_cols, block_cols)
        rows = RING * tok_rows
        out[:, c] = contract_rows(
            left[...].reshape(rows, width), right[:, :, c].reshape(rows, block_cols)
        )

    def mixed_group(m):
        return jnp.concatenate(
            [mixed[m * per + i, core] for core in range(2) for i in range(per)], axis=1
        )

    def group_done(k):
        for h in range(2):
            arrived(mr.at[k, h, 1], mixed.at[k, 1 - here.core, halves[h]])
        if (k + 1) % per:
            return
        m = k // per
        group = mixed_group(m)
        weight = jnp.concatenate(
            [out_ref[pl.ds(d * span + m * atom, atom), :] for d in range(RING)], axis=0
        )
        term = dot(group, weight)
        mixer_cot[...] = term if m == 0 else mixer_cot[...] + term

    def group_proj(m):
        group = mixed_group(m)
        block = dot(group, mixer_out[...], 0, 0).astype(bf16)
        for d in range(RING):
            proj_to[m, d] = block[d * atom : (d + 1) * atom, :]
        for step, device in ((1, here.right), (3, here.left), (2, here.across)):
            go(
                proj_to.at[m, here.at[step]], proj_from.at[m, here.sp],
                js.at[m, step - 1], jr.at[m, 3 - step], device,
            )

    reduce_steps = {
        "pt": lambda m: pair_part(m, everything),
        "op": lambda m: own_part(m, everything),
        "ptb": lambda m: pair_part(m, beside),
        "opb": lambda m: own_part(m, beside),
        "pto": lambda m: pair_part(m, others),
        "opo": lambda m: own_part(m, others),
        "g": weight_grad,
        "rl": ring_relay,
        "to": ring_total,
        "mi": line_middle,
        "lt": line_total,
        "gd": group_done,
        "pj": group_proj,
        "mb": mix_backward,
        "mb2": mix_inner,
        "mb3": mix_outer,
        "mf": mix_finish,
    }
    steps = {**gather_steps, **reduce_steps}
    for name, *rest in GATHER_ORDER + REDUCE_ORDER:
        steps[name](*rest)
    for copy in plain:
        copy.wait_send()
    for cond, copy in guarded:
        @pl.when(cond)
        def _():
            copy.wait_send()


def layer_stage(*inputs):
    x, _, _, _, _, gate, _, _, _, query, key_in, value, logit = inputs
    tok_rows, width = x.shape
    hidden_dev, features = gate.shape
    key_cols, value_cols = query.shape[1], value.shape[1]
    heads = key_cols // DK
    pieces = PIECES
    wide = features // (2 * pieces)
    vmem = pl.BlockSpec(memory_space=pltpu.VMEM)
    dma = pltpu.SemaphoreType.DMA
    f32, bf16 = jnp.float32, jnp.bfloat16
    full = (RING, tok_rows, features)
    acts = (RING, tok_rows, hidden_dev)
    block = (tok_rows, wide)
    state = (key_cols, DV)
    proj = (RING, RING, features // RING**2, value_cols)
    table = (8, -(-max(tok_rows, key_cols) // 128) * 128)
    results = [(hidden_dev, features)] * 3 + [
        (features // RING, value_cols), query.shape, key_in.shape, value.shape, logit.shape
    ]
    return pl.pallas_call(
        layer_kernel,
        out_shape=[jax.ShapeDtypeStruct(shape, f32) for shape in results],
        in_specs=[pl.BlockSpec(memory_space=pltpu.HBM)] * 13,
        out_specs=[vmem] * 8,
        scratch_shapes=[pltpu.VMEM(a.shape, a.dtype) for a in inputs] + [
            dma((len(inputs),)),
            pltpu.VMEM((pieces, 2) + block, bf16),
            pltpu.VMEM(table, f32), pltpu.VMEM((RING,) + table, f32),
            pltpu.VMEM(state, bf16), pltpu.VMEM((RING,) + state, bf16),
            pltpu.VMEM(state, bf16), pltpu.VMEM((RING,) + state, bf16),
            pltpu.VMEM(query.shape, bf16), pltpu.VMEM(query.shape, bf16),
            pltpu.VMEM(query.shape, bf16),
            pltpu.VMEM(state, f32), pltpu.VMEM(state, bf16), pltpu.VMEM(state, f32),
            pltpu.VMEM((heads, tok_rows, tok_rows), bf16),
            pltpu.VMEM(value.shape, bf16), pltpu.VMEM(value.shape, f32),
            pltpu.VMEM(proj, bf16), pltpu.VMEM(proj, bf16),
            pltpu.VMEM(query.shape, f32), pltpu.VMEM(query.shape, f32),
            pltpu.VMEM((RING, tok_rows, 128), f32),
            pltpu.VMEM(full, bf16), pltpu.VMEM(full, bf16),
            pltpu.VMEM(acts, f32), pltpu.VMEM(acts, f32),
            pltpu.VMEM(acts, bf16), pltpu.VMEM(acts, bf16), pltpu.VMEM(acts, bf16),
            pltpu.VMEM((pieces, RING) + block, bf16), pltpu.VMEM((pieces, RING) + block, bf16),
            pltpu.VMEM((pieces, RING) + block, bf16),
            pltpu.VMEM((pieces, 2, tok_rows // 2, wide), bf16),
            pltpu.VMEM((pieces, 2) + block, bf16),
            pltpu.VMEM((pieces,) + block, bf16), pltpu.VMEM((pieces,) + block, bf16),
            pltpu.VMEM((pieces, 2) + block, bf16),
            dma((2, 3)), dma((2, 3)),
            dma((2, 2, 5)), dma((2, 2, 3)),
            dma((2, 5, 6)), dma((2, 5, 6)),
            dma((2, 4, 5)), dma((2, 4, 5)),
            dma((3,)), dma((3,)), dma((RING, 3)), dma((RING, 3)),
            dma((pieces, RING)), dma((pieces, RING)),
            dma((pieces, 2)), dma((pieces, 2)),
            dma((pieces, 4)), dma((pieces, 4)),
            dma((pieces, 2, 2)), dma((pieces, 2, 2)),
            dma((pieces, 2, 2)), dma((pieces, 2, 2)),
        ],
        compiler_params=pltpu.CompilerParams(
            collective_id=0, has_side_effects=True, vmem_limit_bytes=42 << 20
        ),
        name="layer_stage",
    )(*[pltpu.with_memory_space_constraint(a, pltpu.HBM) for a in inputs])


def write_kernel(*refs):
    count = len(refs) // 2
    sems = refs[-1]
    copies = [
        pltpu.make_async_copy(refs[i], refs[count + i], sems.at[i]) for i in range(count)
    ]
    for copy in copies:
        copy.start()
    for copy in copies:
        copy.wait()


def write_out(arrays):
    return pl.pallas_call(
        write_kernel,
        out_shape=[jax.ShapeDtypeStruct(a.shape, a.dtype) for a in arrays],
        in_specs=[pl.BlockSpec(memory_space=pltpu.VMEM)] * len(arrays),
        out_specs=[pl.BlockSpec(memory_space=pltpu.HBM)] * len(arrays),
        scratch_shapes=[pltpu.SemaphoreType.DMA((len(arrays),))],
        compiler_params=pltpu.CompilerParams(vmem_limit_bytes=1 << 20),
        name="write_out",
    )(*arrays)


def ring_local(
    layer_in, out_cot, route_ids, route_probs, group_prob, gate_weight, up_weight,
    down_weight, out_weight, query, key_in, value, decay_logit,
):
    results = write_out(layer_stage(
        layer_in, out_cot, route_ids.T, route_probs.T, group_prob, gate_weight[0], up_weight[0], down_weight[0],
        out_weight, query, key_in, value, decay_logit,
    ))
    return tuple(r[None] for r in results[:3]) + tuple(results[3:])


def solution(mesh):
    in_specs = (
        P("sp", "tp"),
        P("sp", "tp"),
        P("sp", None),
        P("sp", None),
        P("sp"),
        P("sp", "tp", None),
        P("sp", "tp", None),
        P("sp", "tp", None),
        P(None, "tp"),
        P("sp", "tp"),
        P("sp", "tp"),
        P("sp", "tp"),
        P("sp", "tp"),
    )
    out_specs = (
        P("sp", "tp", None),
        P("sp", "tp", None),
        P("sp", "tp", None),
        P("sp", "tp"),
        P("sp", "tp"),
        P("sp", "tp"),
        P("sp", "tp"),
        P("sp", "tp"),
    )
    rows = 4 // mesh.shape["sp"]
    body = ring_local if rows * 4 == 4 and mesh.shape["tp"] == 8 else local
    return jax.shard_map(body, mesh=mesh, in_specs=in_specs, out_specs=out_specs, check_vma=False)
```
